32 devices in a mesh: sp: 4 (over y, x), tp: 8 (over z, core).
Axes of the slice: x: 2, y: 2, z: 4, core: 2. Of those that a mesh axis runs over, the one named last changes fastest.
Arguments:
- queries: bfloat16 [4096, 1024], P('sp', 'tp'), may hold values from -18 to 18
- keys: bfloat16 [4096, 256], P('sp'), may hold values from -18 to 18
- values: bfloat16 [4096, 256], P('sp'), may hold values from -6 to 6
- sink_logits: float32 [16], P('tp'), may hold values from 3 to 7
- w_out: bfloat16 [1024, 2048], P('tp'), may hold values from -1.5 to 1.5
- residual: bfloat16 [4096, 2048], P(('sp', 'tp')), may hold values from -6 to 6
- norm_gain: float32 [2048], replicated, may hold values from 0.1 to 1.9
- expert_ids: int32 [4096, 4], P('sp'), may hold values from 0 to 15, all different within a row; in each aligned block of 1024 rows (0 to 1023, 1024 to 2047, ...) at most 512 rows name the same one
- expert_weights: float32 [4096, 4], P('sp'), may hold values from 0.1 to 1.5
- w_gate: bfloat16 [32, 768, 2048], P(('sp', 'tp')), may hold values from -0.125 to 0.125
- w_up: bfloat16 [32, 768, 2048], P(('sp', 'tp')), may hold values from -0.125 to 0.125
- w_down: bfloat16 [32, 768, 2048], P(('sp', 'tp')), may hold values from -0.15625 to 0.15625
- shared_gate: bfloat16 [512, 2048], P('tp'), may hold values from -0.125 to 0.125
- shared_up: bfloat16 [512, 2048], P('tp'), may hold values from -0.125 to 0.125
- shared_down: bfloat16 [512, 2048], P('tp'), may hold values from -0.25 to 0.25
Outputs:
- layer_out: bfloat16 [4096, 2048], P(('sp', 'tp'))
The draws below stay inside these ranges and needn't reach their ends.
Inputs may be any that keep to these rules, and one draw needn't show every extreme that they name: `expert_ids`: each row names 4 different experts; in each aligned block of 1024 rows no expert is named by more than 512 rows.
All inputs are finite; a program needn't handle non-finite values.
Results may differ from the reference program's by a relative error of at most 0.02.
Values may be sent and summed in bfloat16 or wider, within the bound.
A program may use at most 128 MiB of HBM per device.

```python
import math
import jax
import jax.numpy as jnp
import numpy as np
from jax import lax

D = 2048
HQ = 16
HD = 64
KVH = 4
GROUP = 4
WINDOW = 128
TOK_DEV = 1024
TOKENS = 4096
EXPERTS = 16
TOPK = 4
FF = 1536
SFF = 512
CAP = 512
N_SP = 4
N_TP = 8


def draw_queries(key, part):
    drawn = jnp.clip(jax.random.normal(jax.random.fold_in(key, 11), (TOKENS, HQ * HD), jnp.float32), -6.0, 6.0)
    return drawn.astype(jnp.bfloat16)


def draw_keys(key, part):
    drawn = jnp.clip(jax.random.normal(jax.random.fold_in(key, 23), (TOKENS, KVH * HD), jnp.float32), -6.0, 6.0)
    return drawn.astype(jnp.bfloat16)


def block_levels(key, extent, pieces, low, high):
    def one(dim, blocks):
        heights = jax.random.uniform(jax.random.fold_in(jax.random.fold_in(key, 6), dim), (blocks,), jnp.float32, low / len(pieces), high / len(pieces))
        return jnp.repeat(jnp.exp(heights), extent[dim] // blocks).reshape((-1,) + (1,) * (len(extent) - dim - 1))

    level = one(*pieces[0])
    for cut in pieces[1:]:
        level = level * one(*cut)
    return level


def shared_out(own_key, own, number, rows, count, top, most, slope):
    ranking = jax.random.permutation(own_key, count)
    crowded, common = portions_of(count, rows * top, most, slope, True), portions_of(count, rows * top, most, slope, False)
    places = jnp.arange(count)

    def named(lengths, rotation):
        used = int((lengths > 0).sum())
        fixed = max(1, used // 4)
        shifted = fixed + (places - fixed + rotation * (used - fixed)) % max(1, count - fixed)
        return jnp.zeros((count,), jnp.int32).at[ranking[jnp.where(places < fixed, places, shifted)]].set(jnp.asarray(lengths, jnp.int32))

    lengths = jnp.where(number % 4 == 0, named(crowded, number // 4), named(common, number - number // 4 - 1))
    mixed = jax.random.permutation(jax.random.fold_in(own, 3), count)
    giver, sink = mixed[0:count // 2 * 2:2], mixed[1:count // 2 * 2:2]
    room = jnp.minimum(lengths[giver] - 1, most - lengths[sink]) // 2
    room = jnp.where((giver == ranking[0]) | (sink == ranking[0]) | (lengths[sink] == 0), 0, jnp.maximum(room, 0))
    shifted = jax.random.randint(jax.random.fold_in(own, 4), (count // 2,), 0, 1 << 20) % (room + 1)
    lengths = lengths.at[giver].add(-shifted).at[sink].add(shifted)
    items = jnp.searchsorted(jnp.cumsum(lengths), jnp.arange(rows * top), side="right").astype(jnp.int32)
    listing = items.reshape(top, rows).T
    listing = listing[jax.random.permutation(jax.random.fold_in(own, 1), rows)]
    rotation = jax.random.randint(jax.random.fold_in(own, 2), (rows, 1), 0, top)
    return jnp.take_along_axis(listing, (jnp.arange(top)[None, :] + rotation) % top, axis=1)


def portions_of(amount, total, reach, skew, full):
    portions = [(1 << 20) // math.isqrt(standing ** skew) + 1 for standing in range(1, amount + 1)]
    largest = reach if full else min(reach, max(-(-total // amount), total * portions[0] // sum(portions)))
    least = 1 if total - largest >= amount - 1 else 0
    counts, spare = [largest] + [least] * (amount - 1), total - largest - least * (amount - 1)
    while spare > 0:
        candidates = [i for i in range(1, amount) if counts[i] < largest] or [i for i in range(1, amount) if counts[i] < reach]
        pool, budget = sum([portions[i] for i in candidates]), spare
        for i in candidates:
            addition = min(reach - counts[i], max(1, budget * portions[i] // pool), spare)
            counts[i] = counts[i] + addition
            spare = spare - addition
    return np.array(counts)


def normal_values(rng, shape, width, most, split=(), held_as=jnp.bfloat16):
    gain = block_levels(rng, shape, split, -0.22, 0.18) if split else 1.0
    values = jax.random.normal(rng, shape, jnp.float32) * width * gain
    return jnp.minimum(jnp.maximum(values, -most), most).astype(held_as)


def setup_inputs(seed: int = 0) -> dict:
    key_of = jax.random.split(jax.random.key(seed), 16)
    queries = draw_queries(jax.random.fold_in(key_of[15], 71), 0)
    keys = draw_keys(jax.random.fold_in(key_of[15], 71), 0)
    values = normal_values(key_of[2], (TOKENS, KVH * HD), 1.0, 6.0, ((0, 4),))
    sink_logits = jnp.clip(3.0 + 4.0 * jax.random.uniform(key_of[3], (HQ,), jnp.float32) ** block_levels(key_of[3], (HQ,), ((0, 8),), -0.2, 0.2), 3.0, 7.0)
    w_out = normal_values(key_of[4], (HQ * HD, D), (HQ * HD // 64) ** -0.5, 1.5, ((0, 8),))
    residual = normal_values(key_of[5], (TOKENS, D), 1.0, 6.0, ((0, 32),))
    norm_gain = jnp.clip(1.0 + 0.18 * jax.random.normal(key_of[6], (D,), jnp.float32), 0.1, 1.9)
    expert_ids_keys = jax.random.split(jax.random.fold_in(key_of[7], 1), TOKENS // TOK_DEV)
    expert_ids_turns = jax.random.permutation(jax.random.fold_in(key_of[7], 3), TOKENS // TOK_DEV)
    expert_ids = jax.vmap(lambda own, number: shared_out(jax.random.fold_in(key_of[7], 2), own, number, TOK_DEV, EXPERTS, TOPK, CAP, 2))(expert_ids_keys, expert_ids_turns).reshape((TOKENS, TOPK))
    expert_weights = jnp.clip(jnp.exp(math.log(1.5) - 2.7080502 * jax.random.uniform(key_of[8], (TOKENS, TOPK), jnp.float32) ** block_levels(key_of[8], (TOKENS, TOPK), ((0, 4),), -0.2, 0.2)), 0.1, 1.5)
    w_gate = normal_values(key_of[9], (2 * EXPERTS, FF // 2, D), D ** -0.5, 0.125, ((0, 32),))
    w_up = normal_values(key_of[10], (2 * EXPERTS, FF // 2, D), D ** -0.5, 0.125, ((0, 32),))
    w_down = normal_values(key_of[11], (2 * EXPERTS, FF // 2, D), FF ** -0.5, 0.15625, ((0, 32),))
    shared_gate = normal_values(key_of[12], (SFF, D), D ** -0.5, 0.125, ((0, 8),))
    shared_up = normal_values(key_of[13], (SFF, D), D ** -0.5, 0.125, ((0, 8),))
    shared_down = normal_values(key_of[14], (SFF, D), SFF ** -0.5, 0.25, ((0, 8),))
    return dict(queries=queries, keys=keys, values=values, sink_logits=sink_logits, w_out=w_out, residual=residual, norm_gain=norm_gain, expert_ids=expert_ids, expert_weights=expert_weights, w_gate=w_gate, w_up=w_up, w_down=w_down, shared_gate=shared_gate, shared_up=shared_up, shared_down=shared_down)


def attend(queries, keys, values, sink_logits):
    seq_rows = queries.shape[0]
    num_blocks = seq_rows // WINDOW
    query_blocks = queries.astype(jnp.float32).reshape(num_blocks, WINDOW, KVH, GROUP, HD)
    key_blocks = keys.astype(jnp.float32).reshape(num_blocks, WINDOW, KVH, HD)
    value_blocks = values.astype(jnp.float32).reshape(num_blocks, WINDOW, KVH, HD)

    def shift_back(blocks):
        return jnp.concatenate([jnp.zeros_like(blocks[:1]), blocks[:-1]], axis=0)
    keys_ext = jnp.concatenate([shift_back(key_blocks), key_blocks], axis=1)
    values_ext = jnp.concatenate([shift_back(value_blocks), value_blocks], axis=1)
    scores = jnp.einsum('nqhgd,nshd->nhgqs', query_blocks, keys_ext) * HD ** (-0.5)
    query_pos = jnp.arange(WINDOW)[:, None] + WINDOW
    key_pos = jnp.arange(2 * WINDOW)[None, :]
    in_band = (key_pos <= query_pos) & (key_pos > query_pos - WINDOW)
    absolute = jnp.arange(num_blocks)[:, None, None] * WINDOW + key_pos[None] - WINDOW
    allowed = in_band[None] & (absolute >= 0)
    scores = jnp.where(allowed[:, None, None], scores, -jnp.inf)
    sink_col = jnp.broadcast_to(sink_logits.reshape(KVH, GROUP)[None, :, :, None, None], scores.shape[:-1] + (1,))
    combined = jnp.concatenate([scores, sink_col], axis=-1)
    row_max = lax.optimization_barrier(jnp.max(combined, axis=-1, keepdims=True))
    exps = jnp.exp(combined - row_max)
    weights = (exps[..., :-1] / lax.optimization_barrier(jnp.sum(exps, axis=-1, keepdims=True))).astype(jnp.bfloat16)
    attended = jnp.einsum('nhgqs,nshd->nqhgd', weights.astype(jnp.float32), values_ext)
    return attended.astype(jnp.bfloat16).reshape(seq_rows, HQ * HD)

def normalize(after_mix, norm_gain):
    values_f = after_mix.astype(jnp.float32)
    scale = lax.rsqrt(lax.optimization_barrier(jnp.mean(values_f * values_f, axis=-1, keepdims=True)) + 1e-06)
    return (values_f * scale * norm_gain).astype(jnp.bfloat16)

def slot_layout(route_ids):
    flat_ids = route_ids.reshape(-1).astype(jnp.int32)
    matches = (flat_ids[:, None] == jnp.arange(EXPERTS, dtype=jnp.int32)[None, :]).astype(jnp.int32)
    earlier = jnp.cumsum(matches, axis=0).astype(jnp.int32) - matches
    order_in = lax.optimization_barrier(jnp.sum(earlier * matches, axis=1)).astype(jnp.int32)
    slot_index = flat_ids * CAP + order_in
    owners = jnp.arange(flat_ids.shape[0], dtype=jnp.int32) // TOPK
    slot_owner = jnp.full((EXPERTS * CAP,), -1, jnp.int32).at[slot_index].set(owners)
    return (slot_index, slot_owner)

def run_expert(operands):
    row_block, gate_w, up_w, down_w = operands
    total = jnp.zeros((row_block.shape[0], D), jnp.float32)
    for half in range(2):
        gate_act = jnp.dot(row_block, gate_w[half].T, preferred_element_type=jnp.float32)
        up_act = jnp.dot(row_block, up_w[half].T, preferred_element_type=jnp.float32)
        hidden = (jax.nn.silu(gate_act) * up_act).astype(jnp.bfloat16)
        term = jnp.dot(hidden, down_w[half], preferred_element_type=jnp.float32).astype(jnp.bfloat16)
        term = lax.optimization_barrier(term)
        total = total + term.astype(jnp.float32)
    return total.astype(jnp.bfloat16)

def reference(queries, keys, values, sink_logits, w_out, residual, norm_gain, expert_ids, expert_weights, w_gate, w_up, w_down, shared_gate, shared_up, shared_down):
    attended = attend(queries, keys, values, sink_logits)
    projected = jnp.dot(attended, w_out, preferred_element_type=jnp.float32)
    after_mix = (residual.astype(jnp.float32) + projected).astype(jnp.bfloat16)
    normed = normalize(after_mix, norm_gain)
    block_rows = normed.reshape(N_SP, TOK_DEV, D)
    block_ids = expert_ids.reshape(N_SP, TOK_DEV, TOPK)
    slot_index, slot_owner = jax.vmap(slot_layout)(block_ids)

    def fill_slots(rows_here, owner_here):
        picked = rows_here[jnp.maximum(owner_here, 0)]
        return jnp.where((owner_here >= 0)[:, None], picked, jnp.zeros((), jnp.bfloat16))
    slot_rows = jax.vmap(fill_slots)(block_rows, slot_owner)
    per_expert = jnp.transpose(slot_rows.reshape(N_SP, EXPERTS, CAP, D), (1, 0, 2, 3)).reshape(EXPERTS, N_SP * CAP, D)
    gate_pieces = w_gate.reshape(EXPERTS, 2, FF // 2, D)
    up_pieces = w_up.reshape(EXPERTS, 2, FF // 2, D)
    down_pieces = w_down.reshape(EXPERTS, 2, FF // 2, D)
    expert_out = lax.map(run_expert, (per_expert, gate_pieces, up_pieces, down_pieces))
    returned = jnp.transpose(expert_out.reshape(EXPERTS, N_SP, CAP, D), (1, 0, 2, 3)).reshape(N_SP, EXPERTS * CAP, D)
    shared_hidden = (jax.nn.silu(jnp.dot(normed, shared_gate.T, preferred_element_type=jnp.float32)) * jnp.dot(normed, shared_up.T, preferred_element_type=jnp.float32)).astype(jnp.bfloat16)
    lanes = N_TP // 2
    half_cap = CAP // 2
    unit_width = SFF // N_TP

    def block_moe(operands):
        outputs, index_flat, ids, wts, hidden_rows = operands
        index_pairs = index_flat.reshape(TOK_DEV, TOPK)
        rank = index_pairs - ids * CAP
        group = 2 * (ids % lanes) + rank // half_cap
        chosen = [outputs[index_pairs[:, k]].astype(jnp.float32) for k in range(TOPK)]

        def add_group(total, group_id):
            part = jnp.zeros((TOK_DEV, D), jnp.float32)
            for k in range(TOPK):
                factor = jnp.where(group[:, k] == group_id, wts[:, k], jnp.zeros((), wts.dtype))
                part = part + factor[:, None] * chosen[k]
            hid = lax.dynamic_slice_in_dim(hidden_rows, group_id * unit_width, unit_width, 1)
            down = lax.dynamic_slice_in_dim(shared_down, group_id * unit_width, unit_width, 0)
            part = part + jnp.dot(hid, down, preferred_element_type=jnp.float32)
            rounded = lax.optimization_barrier(part.astype(jnp.bfloat16))
            return (total + rounded.astype(jnp.float32), None)
        total, _ = lax.scan(add_group, jnp.zeros((TOK_DEV, D), jnp.float32), jnp.arange(N_TP, dtype=jnp.int32))
        return total.astype(jnp.bfloat16)
    moe_out = lax.map(block_moe, (returned, slot_index, block_ids, expert_weights.reshape(N_SP, TOK_DEV, TOPK), shared_hidden.reshape(N_SP, TOK_DEV, SFF)))
    moe_out = moe_out.reshape(TOKENS, D)
    return (after_mix.astype(jnp.float32) + moe_out.astype(jnp.float32)).astype(jnp.bfloat16)
```

```python
import functools

import jax
import jax.numpy as jnp
from jax import lax
from jax.experimental import pallas as pl
from jax.experimental.pallas import tpu as pltpu
from jax.sharding import PartitionSpec as P

HD = 64
GROUP = 4
WINDOW = 128
TOPK = 4
CHUNKS = 4
TILE = 256
MESH = pl.DeviceIdType.MESH
F32 = jnp.float32
BF16 = jnp.bfloat16
NT = (((1,), (1,)), ((), ()))


def dot(a, b):
    return jnp.dot(a, b, preferred_element_type=F32)


def dot_t(a, b):
    return lax.dot_general(a, b, NT, preferred_element_type=F32)


def silu(v):
    return v / (1.0 + jnp.exp(jnp.minimum(-v, 87.0)))


def loop(n, body):
    lax.fori_loop(0, n, lambda i, carry: (body(i), carry)[1], 0)


def moe_kernel(
    normed,
    after_mix,
    place_t,
    place,
    weight,
    w_gate,
    w_up,
    w_down,
    s_gate,
    s_up,
    s_down,
    out,
    wg,
    wu,
    wd,
    sgu,
    sd,
    gathered,
    onehot,
    mix,
    sent,
    arrived,
    acc_g,
    acc_u,
    sh_acc,
    sh,
    returned,
    x_recv,
    z_recv,
    w_sem,
    pw_send,
    pw_recv,
    s_sem,
    ag_send,
    ag_recv,
    fw_send,
    fw_recv,
    d_send,
    d_recv,
    r_send,
    r_recv,
    x_ssem,
    x_rsem,
    z_ssem,
    z_rsem,
):
    n_sp = lax.axis_size("sp")
    n_tp = lax.axis_size("tp")
    lanes = n_tp // 2
    s = lax.axis_index("sp")
    t = lax.axis_index("tp")
    z = t // 2
    core = t % 2
    rows = normed.shape[0]
    chunks, _, _, step = gathered.shape
    half_cap = sent.shape[2]
    slots = n_sp * half_cap
    ff = wg.shape[1] // 2
    sff = sd.shape[1]
    bands = 2 * ff // TILE
    per = step // TILE

    def sp_peer(j):
        return {"sp": (s + j) % n_sp}

    def z_peer(j):
        return {"tp": ((z + j) % lanes) * 2 + core}

    partner = {"tp": z * 2 + 1 - core}

    barrier = pltpu.get_barrier_semaphore()
    for j in range(1, n_sp):
        pl.semaphore_signal(barrier, inc=1, device_id=sp_peer(j), device_id_type=MESH)
    for j in range(1, lanes):
        pl.semaphore_signal(barrier, inc=1, device_id=z_peer(j), device_id_type=MESH)
    pl.semaphore_signal(barrier, inc=1, device_id=partner, device_id_type=MESH)
    pl.semaphore_wait(barrier, n_sp - 1 + lanes - 1 + 1)

    def cols(c):
        return pl.ds(pl.multiple_of(c * step, step), step)

    def remote(src, dst, send, recv, peer):
        return pltpu.make_async_remote_copy(
            src_ref=src, dst_ref=dst, send_sem=send, recv_sem=recv, device_id=peer, device_id_type=MESH
        )

    def own_piece(c, j):
        return remote(normed.at[:, cols(c)], gathered.at[c, t], ag_send.at[c, j], ag_recv.at[c, j], z_peer(j))

    def own_to_partner(c):
        return remote(normed.at[:, cols(c)], gathered.at[c, t], fw_send.at[c, 0], fw_recv.at[c, 0], partner)

    def forward(c, j):
        src = gathered.at[c, ((z + lanes - j) % lanes) * 2 + core]
        return remote(src, src, fw_send.at[c, j], fw_recv.at[c, j], partner)

    def dispatch(c, j):
        return remote(sent.at[c, j], arrived.at[c, j], d_send.at[c, j], d_recv.at[c, j], sp_peer(j))

    def give_back(c, j):
        return remote(
            sent.at[c, j], returned.at[c, j], r_send.at[c, j], r_recv.at[c, j], sp_peer(n_sp - j)
        )

    def cross(c):
        return remote(gathered.at[c, 0:lanes], x_recv.at[c], x_ssem.at[c], x_rsem.at[c], partner)

    def spread(c, j):
        return remote(gathered.at[c, lanes + j], z_recv.at[c, j], z_ssem.at[c, j], z_rsem.at[c, j], z_peer(j))

    weights = ((w_gate, wg), (w_up, wu), (w_down, wd))
    shared = (
        (s_gate, lambda c: sgu.at[c, 0:sff]),
        (s_up, lambda c: sgu.at[c, sff : 2 * sff]),
        (s_down, lambda c: sd.at[c]),
    )

    def own_weight(n, c):
        src, dst = weights[n]
        return pltpu.make_async_copy(src.at[0, :, cols(c)], dst.at[c, 0:ff], w_sem.at[n, c])

    def other_weight(n, c):
        src, dst = weights[n]
        return remote(src.at[0, :, cols(c)], dst.at[c, ff : 2 * ff], pw_send.at[n, c], pw_recv.at[n, c], partner)

    def shared_weight(n, c):
        src, dst = shared[n]
        return pltpu.make_async_copy(src.at[:, cols(c)], dst(c), s_sem.at[n, c])

    def start_sends(c):
        for j in range(1, lanes):
            own_piece(c, j).start()
        own_to_partner(c).start()

    loop(chunks, start_sends)

    def start_weights(c):
        for n in range(2):
            own_weight(n, c).start()
            other_weight(n, c).start()
            shared_weight(n, c).start()

    loop(chunks, start_weights)

    def start_down(c):
        own_weight(2, c).start()
        other_weight(2, c).start()
        shared_weight(2, c).start()

    loop(chunks, start_down)

    def keep_own(c):
        gathered[c, t] = normed[:, cols(c)]

    loop(chunks, keep_own)

    slot_down = lax.broadcasted_iota(jnp.int32, (half_cap, 1), 0).astype(F32)
    slot_along = lax.broadcasted_iota(jnp.int32, (1, half_cap), 1).astype(F32)

    def build_pick(j):
        hit = place_t[j] == slot_down
        onehot[j] = jnp.where(hit, 1.0, 0.0).astype(BF16)

    loop(n_sp, build_pick)

    def build_mix(i):
        for j in range(n_sp):
            hit = place[i, :, j : j + 1] == slot_along
            part = jnp.where(hit, weight[i, :, j : j + 1], 0.0).astype(BF16)
            mix[i, :, j * half_cap : (j + 1) * half_cap] = part

    loop(n_tp, build_mix)

    def gather_chunk(c):
        for j in range(1, lanes):
            own_piece(c, j).wait_recv()
            forward(c, j).start()
        own_to_partner(c).wait_recv()
        for j in range(1, lanes):
            forward(c, j).wait_recv()

    def pick_chunk(c):
        block = gathered[c].reshape(n_tp * rows, step)

        def one(i):
            j = (i + 1) % n_sp
            value = dot(onehot[j], block).astype(BF16)

            @pl.when(j > 0)
            def _():
                sent[c, j] = value
                dispatch(c, j).start()

            @pl.when(j == 0)
            def _():
                arrived[c, j] = value

        loop(n_sp, one)

    def shared_chunk(c):
        for n in range(2):
            shared_weight(n, c).wait()
        block = gathered[c].reshape(n_tp * rows, step)
        value = dot_t(block, sgu[c])

        @pl.when(c == 0)
        def _():
            sh_acc[...] = value

        @pl.when(c > 0)
        def _():
            sh_acc[...] += value

    def expert_chunk(c):
        for n in range(2):
            own_weight(n, c).wait()
            other_weight(n, c).wait_recv()

        for j in range(1, n_sp):
            dispatch(c, j).wait_recv()
        lhs = arrived[c].reshape(slots, step)

        def one(i):
            band = pl.ds(pl.multiple_of(i * TILE, TILE), TILE)
            for w, acc in ((wg, acc_g), (wu, acc_u)):
                value = dot_t(lhs, w[c, band, :])

                @pl.when(c == 0)
                def _():
                    acc[i] = value

                @pl.when(c > 0)
                def _():
                    acc[i] += value

        loop(bands, one)

    def dispatch_step(c):
        gather_chunk(c)
        pick_chunk(c)
        shared_chunk(c)

        @pl.when(c > 0)
        def _():
            expert_chunk(c - 1)

    loop(chunks, dispatch_step)
    expert_chunk(chunks - 1)

    def activate(i):
        value = (silu(acc_g[i]) * acc_u[i]).astype(BF16).reshape(n_sp, half_cap, TILE)
        band = pl.ds(pl.multiple_of(i % per * TILE, TILE), TILE)
        arrived[i // per, :, :, band] = value

    loop(bands, activate)
    shared_value = silu(sh_acc[:, 0:sff]) * sh_acc[:, sff : 2 * sff]
    sh[...] = shared_value.astype(BF16).reshape(sh.shape)

    def settle_dispatch(c):
        for j in range(1, n_sp):
            dispatch(c, j).wait_send()
        for j in range(1, lanes):
            forward(c, j).wait_send()

    loop(chunks, settle_dispatch)

    def down_chunk(c):
        own_weight(2, c).wait()
        other_weight(2, c).wait_recv()

        def one(i):
            j = (i + 1) % n_sp
            parts = [
                dot(arrived[n, j], wd[c, n * step : (n + 1) * step, :]) for n in range(2 * ff // step)
            ]
            value = sum(parts[1:], parts[0]).astype(BF16)

            @pl.when(j > 0)
            def _():
                sent[c, j] = value
                give_back(c, j).start()

            @pl.when(j == 0)
            def _():
                returned[c, j] = value

        loop(n_sp, one)

    loop(chunks, down_chunk)

    def combine_chunk(c):
        shared_weight(2, c).wait()
        for j in range(1, n_sp):
            give_back(c, j).wait_recv()
        held = returned[c].reshape(slots, step)

        def part(i):
            return dot(mix[i], held) + dot(sh[i], sd[c])

        def away(i):
            gathered[c, i] = part(i * 2 + 1 - core).astype(BF16)

        loop(lanes, away)
        cross(c).start()
        cross(c).wait_recv()

        def home(i):
            j = (i + 1) % lanes
            other = (z + j) % lanes
            value = part(other * 2 + core) + x_recv[c, other].astype(F32)
            gathered[c, lanes + j] = value.astype(BF16)

            @pl.when(j > 0)
            def _():
                spread(c, j).start()

        loop(lanes, home)

    loop(chunks, combine_chunk)

    def finish_chunk(c):
        total = gathered[c, lanes].astype(F32)
        for j in range(1, lanes):
            spread(c, j).wait_recv()
        for j in range(1, lanes):
            total += z_recv[c, j].astype(F32)
        out[:, cols(c)] = (after_mix[:, cols(c)].astype(F32) + total).astype(BF16)

    loop(chunks, finish_chunk)

    def settle(c):
        for j in range(1, lanes):
            own_piece(c, j).wait_send()
            spread(c, j).wait_send()
        own_to_partner(c).wait_send()
        for j in range(1, n_sp):
            give_back(c, j).wait_send()
        for n in range(3):
            other_weight(n, c).wait_send()
        cross(c).wait_send()

    loop(chunks, settle)


def moe(normed, after_mix, place_t, place, weight, w_gate, w_up, w_down, s_gate, s_up, s_down):
    n_sp = lax.axis_size("sp")
    n_tp = lax.axis_size("tp")
    lanes = n_tp // 2
    rows, width = normed.shape
    step = width // CHUNKS
    ff = w_gate.shape[1]
    sff = s_gate.shape[0]
    q = rows * n_tp
    half_cap = max(2, 2 * q * TOPK // (n_sp * lanes)) // 2
    slots = n_sp * half_cap
    dma = pltpu.SemaphoreType.DMA
    vm = pltpu.VMEM
    in_vmem = pl.BlockSpec(memory_space=pltpu.VMEM)
    in_hbm = pl.BlockSpec(memory_space=pl.ANY)
    scratch = [
        vm((CHUNKS, 2 * ff, step), BF16),
        vm((CHUNKS, 2 * ff, step), BF16),
        vm((CHUNKS, 2 * ff, step), BF16),
        vm((CHUNKS, 2 * sff, step), BF16),
        vm((CHUNKS, sff, step), BF16),
        vm((CHUNKS, n_tp, rows, step), BF16),
        vm((n_sp, half_cap, q), BF16),
        vm((n_tp, rows, slots), BF16),
        vm((CHUNKS, n_sp, half_cap, step), BF16),
        vm((CHUNKS, n_sp, half_cap, step), BF16),
        vm((2 * ff // TILE, slots, TILE), F32),
        vm((2 * ff // TILE, slots, TILE), F32),
        vm((q, 2 * sff), F32),
        vm((n_tp, rows, sff), BF16),
        vm((CHUNKS, n_sp, half_cap, step), BF16),
        vm((CHUNKS, lanes, rows, step), BF16),
        vm((CHUNKS, lanes, rows, step), BF16),
        dma((3, CHUNKS)),
        dma((3, CHUNKS)),
        dma((3, CHUNKS)),
        dma((3, CHUNKS)),
        dma((CHUNKS, lanes)),
        dma((CHUNKS, lanes)),
        dma((CHUNKS, lanes)),
        dma((CHUNKS, lanes)),
        dma((CHUNKS, n_sp)),
        dma((CHUNKS, n_sp)),
        dma((CHUNKS, n_sp)),
        dma((CHUNKS, n_sp)),
        dma((CHUNKS,)),
        dma((CHUNKS,)),
        dma((CHUNKS, lanes)),
        dma((CHUNKS, lanes)),
    ]
    return pl.pallas_call(
        moe_kernel,
        name="moe",
        out_shape=jax.ShapeDtypeStruct((rows, width), BF16),
        in_specs=[in_vmem] * 5 + [in_hbm] * 6,
        out_specs=in_vmem,
        scratch_shapes=scratch,
        compiler_params=pltpu.CompilerParams(
            collective_id=0, has_side_effects=True, vmem_limit_bytes=67043328
        ),
        cost_estimate=pl.CostEstimate(
            flops=12 * slots * ff * width, bytes_accessed=6 * ff * width, transcendentals=0
        ),
    )(normed, after_mix, place_t, place, weight, w_gate, w_up, w_down, s_gate, s_up, s_down)


def shifted(block, axis, distance):
    devices = range(lax.axis_size(axis))
    route = [(i - distance, i) for i in devices if i - distance in devices]
    return lax.ppermute(block, axis, route)


def normalize(after_mix, norm_gain):
    values_f = after_mix.astype(F32)
    scale = lax.rsqrt(jnp.mean(values_f * values_f, axis=-1, keepdims=True) + 1e-06)
    return (values_f * scale * norm_gain).astype(BF16)


def slot_places(route_ids, route_weights, targets, first_rank):
    named = route_ids[:, :, None] == targets[None, None, :]
    named_f = jnp.sum(named.astype(F32), axis=1)
    weight = jnp.sum(jnp.where(named, route_weights[:, :, None], 0.0), axis=1)
    rows = route_ids.shape[0]
    steps = jnp.arange(rows)
    earlier = (steps[None, :] < steps[:, None]).astype(BF16)
    rank = jnp.dot(earlier, named_f.astype(BF16), preferred_element_type=F32)
    place = jnp.where(named_f > 0, rank - first_rank, -1.0)
    return place, weight


def body(
    queries,
    keys,
    values,
    sink_logits,
    w_out,
    residual,
    norm_gain,
    expert_ids,
    expert_weights,
    w_gate,
    w_up,
    w_down,
    shared_gate,
    shared_up,
    shared_down,
):
    tp_count = lax.axis_size("tp")
    sp_count = lax.axis_size("sp")
    seq_rows = queries.shape[0]
    expert_count = sp_count * tp_count // 2
    capacity = max(2, 2 * seq_rows * TOPK // expert_count)
    local_heads = queries.shape[1] // HD
    kv_start = lax.axis_index("tp") * local_heads // GROUP * HD
    key_cols = lax.dynamic_slice_in_dim(keys, kv_start, HD, 1)
    value_cols = lax.dynamic_slice_in_dim(values, kv_start, HD, 1)
    rim = jnp.concatenate([keys[seq_rows - WINDOW :], values[seq_rows - WINDOW :]], axis=1)
    rim = shifted(rim, "sp", 1)
    rim_keys = lax.dynamic_slice_in_dim(rim, kv_start, HD, 1)
    rim_values = lax.dynamic_slice_in_dim(rim, kv_start + keys.shape[1], HD, 1)
    num_blocks = seq_rows // WINDOW
    key_blocks = key_cols.reshape(num_blocks, WINDOW, HD)
    value_blocks = value_cols.reshape(num_blocks, WINDOW, HD)
    keys_ext = jnp.concatenate(
        [jnp.concatenate([rim_keys[None], key_blocks[:-1]], axis=0), key_blocks], axis=1
    )
    values_ext = jnp.concatenate(
        [jnp.concatenate([rim_values[None], value_blocks[:-1]], axis=0), value_blocks], axis=1
    )
    query_blocks = queries.reshape(num_blocks, WINDOW, local_heads, HD)
    scores = jnp.einsum(
        "nqhd,nsd->nhqs", query_blocks, keys_ext, preferred_element_type=F32
    ) * HD ** (-0.5)
    query_pos = jnp.arange(WINDOW)[:, None] + WINDOW
    key_pos = jnp.arange(2 * WINDOW)[None, :]
    in_band = (key_pos <= query_pos) & (key_pos > query_pos - WINDOW)
    absolute = (
        lax.axis_index("sp") * seq_rows
        + jnp.arange(num_blocks)[:, None, None] * WINDOW
        + key_pos[None]
        - WINDOW
    )
    allowed = in_band[None] & (absolute >= 0)
    scores = jnp.where(allowed[:, None], scores, -jnp.inf)
    sink_col = jnp.broadcast_to(sink_logits[None, :, None, None], scores.shape[:-1] + (1,))
    combined = jnp.concatenate([scores, sink_col], axis=-1)
    row_max = jnp.max(combined, axis=-1, keepdims=True)
    exps = jnp.exp(combined - row_max)
    weights = (exps[..., :-1] / jnp.sum(exps, axis=-1, keepdims=True)).astype(BF16)
    attended = jnp.einsum("nhqs,nsd->nqhd", weights, values_ext, preferred_element_type=F32)
    attended = attended.astype(BF16).reshape(seq_rows, local_heads * HD)
    head_rows = lax.all_to_all(attended, "tp", split_axis=0, concat_axis=1, tiled=True)
    projected = jnp.dot(
        head_rows,
        lax.all_gather(w_out, "tp", axis=0, tiled=True),
        preferred_element_type=F32,
    )
    after_mix = (residual.astype(F32) + projected).astype(BF16)
    normed = normalize(after_mix, norm_gain)
    tp_index = lax.axis_index("tp")
    sp_index = lax.axis_index("sp")
    lanes = tp_count // 2
    lane = tp_index // 2
    half_cap = capacity // 2
    columns = (jnp.arange(sp_count, dtype=jnp.int32) + sp_index) % sp_count
    targets = columns * lanes + lane
    first_rank = (tp_index % 2 * half_cap).astype(F32)
    place, weight = slot_places(expert_ids, expert_weights, targets, first_rank)
    rows = after_mix.shape[0]
    return moe(
        normed,
        after_mix,
        place.T.reshape(sp_count, 1, seq_rows),
        place.reshape(tp_count, rows, sp_count),
        weight.reshape(tp_count, rows, sp_count),
        w_gate,
        w_up,
        w_down,
        shared_gate,
        shared_up,
        shared_down,
    )


def solution(mesh):
    return jax.shard_map(
        body,
        mesh=mesh,
        in_specs=(
            P("sp", "tp"),
            P("sp", None),
            P("sp", None),
            P("tp"),
            P("tp", None),
            P(("sp", "tp"), None),
            P(),
            P("sp", None),
            P("sp", None),
            P(("sp", "tp"), None, None),
            P(("sp", "tp"), None, None),
            P(("sp", "tp"), None, None),
            P("tp", None),
            P("tp", None),
            P("tp", None),
        ),
        out_specs=P(("sp", "tp"), None),
        check_vma=False,
    )
```

```python
import functools

import jax
import jax.numpy as jnp
from jax import lax
from jax.experimental import pallas as pl
from jax.experimental.pallas import tpu as pltpu
from jax.sharding import PartitionSpec as P

HD = 64
GROUP = 4
WINDOW = 128
TOPK = 4
CHUNKS = 4
TILE = 256
MESH = pl.DeviceIdType.MESH
F32 = jnp.float32
BF16 = jnp.bfloat16
NT = (((1,), (1,)), ((), ()))


def dot(a, b):
    return jnp.dot(a, b, preferred_element_type=F32)


def dot_t(a, b):
    return lax.dot_general(a, b, NT, preferred_element_type=F32)


def silu(v):
    return v / (1.0 + jnp.exp(jnp.minimum(-v, 87.0)))


def loop(n, body):
    lax.fori_loop(0, n, lambda i, carry: (body(i), carry)[1], 0)


def layer_kernel(
    queries,
    sinks,
    info,
    gain,
    keys,
    values,
    w_out,
    residual,
    w_gate,
    w_up,
    w_down,
    s_gate,
    s_up,
    s_down,
    out,
    wg,
    wu,
    wd,
    sgu,
    sd,
    gathered,
    onehot,
    mix,
    sent,
    arrived,
    acc_g,
    acc_u,
    sh_acc,
    sh,
    returned,
    x_recv,
    z_recv,
    w_sem,
    pw_send,
    pw_recv,
    s_sem,
    ag_send,
    ag_recv,
    fw_send,
    fw_recv,
    d_send,
    d_recv,
    r_send,
    r_recv,
    x_ssem,
    x_rsem,
    z_ssem,
    z_rsem,
    k_ext,
    v_ext,
    attended,
    heads,
    after_mix,
    place_t,
    place,
    weight,
    l_sem,
    rim_send,
    rim_recv,
    wz_send,
    wz_recv,
    wx_send,
    wx_recv,
    h_send,
    h_recv,
    p_send,
    p_recv,
):
    n_sp = lax.axis_size("sp")
    n_tp = lax.axis_size("tp")
    lanes = n_tp // 2
    s = lax.axis_index("sp")
    t = lax.axis_index("tp")
    z = t // 2
    core = t % 2
    rows = after_mix.shape[0]
    width = after_mix.shape[1]
    head_cols = w_out.shape[0]
    seq_rows = n_tp * rows
    chunks, _, _, step = gathered.shape
    half_cap = sent.shape[2]
    slots = n_sp * half_cap
    ff = wg.shape[1] // 2
    sff = sd.shape[1]
    bands = 2 * ff // TILE
    per = step // TILE

    def sp_peer(j):
        return {"sp": (s + j) % n_sp}

    def z_peer(j):
        return {"tp": ((z + j) % lanes) * 2 + core}

    partner = {"tp": z * 2 + 1 - core}

    barrier = pltpu.get_barrier_semaphore()
    for j in range(1, n_sp):
        pl.semaphore_signal(barrier, inc=1, device_id=sp_peer(j), device_id_type=MESH)
    for j in range(1, lanes):
        pl.semaphore_signal(barrier, inc=1, device_id=z_peer(j), device_id_type=MESH)
    pl.semaphore_signal(barrier, inc=1, device_id=partner, device_id_type=MESH)
    pl.semaphore_wait(barrier, n_sp - 1 + lanes - 1 + 1)

    def cols(c):
        return pl.ds(pl.multiple_of(c * step, step), step)

    def remote(src, dst, send, recv, peer):
        return pltpu.make_async_remote_copy(
            src_ref=src, dst_ref=dst, send_sem=send, recv_sem=recv, device_id=peer, device_id_type=MESH
        )

    def own_piece(c, j):
        return remote(gathered.at[c, t], gathered.at[c, t], ag_send.at[c, j], ag_recv.at[c, j], z_peer(j))

    def own_to_partner(c):
        return remote(gathered.at[c, t], gathered.at[c, t], fw_send.at[c, 0], fw_recv.at[c, 0], partner)

    def forward(c, j):
        src = gathered.at[c, ((z + lanes - j) % lanes) * 2 + core]
        return remote(src, src, fw_send.at[c, j], fw_recv.at[c, j], partner)

    def dispatch(c, j):
        return remote(sent.at[c, j], arrived.at[c, j], d_send.at[c, j], d_recv.at[c, j], sp_peer(j))

    def give_back(c, j):
        return remote(
            sent.at[c, j], returned.at[c, j], r_send.at[c, j], r_recv.at[c, j], sp_peer(n_sp - j)
        )

    def cross(c):
        return remote(gathered.at[c, 0:lanes], x_recv.at[c], x_ssem.at[c], x_rsem.at[c], partner)

    def spread(c, j):
        return remote(gathered.at[c, lanes + j], z_recv.at[c, j], z_ssem.at[c, j], z_rsem.at[c, j], z_peer(j))

    weights = ((w_gate, wg), (w_up, wu), (w_down, wd))
    shared = (
        (s_gate, lambda c: sgu.at[c, 0:sff]),
        (s_up, lambda c: sgu.at[c, sff : 2 * sff]),
        (s_down, lambda c: sd.at[c]),
    )

    def own_weight(n, c):
        src, dst = weights[n]
        return pltpu.make_async_copy(src.at[0, :, cols(c)], dst.at[c, 0:ff], w_sem.at[n, c])

    def other_weight(n, c):
        src, dst = weights[n]
        return remote(src.at[0, :, cols(c)], dst.at[c, ff : 2 * ff], pw_send.at[n, c], pw_recv.at[n, c], partner)

    def shared_weight(n, c):
        src, dst = shared[n]
        return pltpu.make_async_copy(src.at[:, cols(c)], dst(c), s_sem.at[n, c])

    group_width = min(width // n_sp, step)
    groups = width // group_width // n_sp

    def group_at(sp, g, lane):
        first = (sp * groups + g) * group_width
        band = pl.ds(pl.multiple_of(first % step, group_width), group_width)
        return wd.at[first // step, pl.ds(pl.multiple_of(lane * head_cols, head_cols), head_cols), band]

    def group_of_mine(g):
        first = (s * groups + g) * group_width
        return w_out.at[:, pl.ds(pl.multiple_of(first, group_width), group_width)]

    def out_shard(g, j):
        return remote(group_of_mine(g), group_at(s, g, z), wz_send.at[g, j], wz_recv.at[g, j], z_peer(j))

    def out_relay(g, j, i):
        block = group_at(s, g, (z + lanes - j) % lanes)
        return remote(block, block, wx_send.at[g, j, i], wx_recv.at[g, j, i], sp_peer(i))

    def out_own(c):
        mine = wd.at[c, pl.ds(pl.multiple_of(z * head_cols, head_cols), head_cols)]
        return pltpu.make_async_copy(w_out.at[:, cols(c)], mine, l_sem.at[3, c])

    kv_start = t * head_cols // HD // GROUP * HD
    kv_cols = pl.ds(pl.multiple_of(kv_start // 128 * 128, 128), 128)
    parity = kv_start // HD % 2

    def rim(src, dst, n):
        last = src.at[pl.ds(seq_rows - WINDOW, WINDOW), kv_cols]
        return remote(last, dst.at[0:WINDOW], rim_send.at[n], rim_recv.at[n], sp_peer(1))

    def own_kv(src, dst, n):
        return pltpu.make_async_copy(src.at[:, kv_cols], dst.at[WINDOW : WINDOW + seq_rows], l_sem.at[n, 0])

    own_residual = pltpu.make_async_copy(residual, after_mix, l_sem.at[2, 0])
    rim(keys, k_ext, 0).start()
    rim(values, v_ext, 1).start()
    own_kv(keys, k_ext, 0).start()
    own_kv(values, v_ext, 1).start()
    for g in range(groups):
        for j in range(1, lanes):
            out_shard(g, j).start()
    own_residual.start()

    def start_weights(c):
        out_own(c).start()
        for n in range(2):
            own_weight(n, c).start()
            other_weight(n, c).start()
            shared_weight(n, c).start()
        other_weight(2, c).start()
        shared_weight(2, c).start()

    own_kv(keys, k_ext, 0).wait()
    own_kv(values, v_ext, 1).wait()
    loop(chunks, start_weights)
    rim(keys, k_ext, 0).wait_recv()
    rim(values, v_ext, 1).wait_recv()

    lane_id = lax.broadcasted_iota(jnp.int32, (1, 128), 1)
    query_row = lax.broadcasted_iota(jnp.int32, (2 * rows, 1), 0)
    in_block = query_row % rows
    key_at = lax.broadcasted_iota(jnp.int32, (1, rows + WINDOW), 1)
    band_mask = (key_at <= in_block + WINDOW) & (key_at > in_block)
    sink = jnp.where(query_row < rows, sinks[0], sinks[1])

    def attend(block):
        first = pl.multiple_of(block * rows, rows)
        q = queries[pl.ds(first, rows), :].astype(F32) * HD ** (-0.5)
        turned = pltpu.roll(q, 64, 1)
        mine = lane_id // HD == parity
        q0 = jnp.where(mine, jnp.where(parity == 0, q, turned), 0.0)
        q1 = jnp.where(mine, jnp.where(parity == 1, q, turned), 0.0)
        q2 = jnp.concatenate([q0, q1], axis=0).astype(BF16)
        scores = dot_t(q2, k_ext[pl.ds(first, rows + WINDOW), :])
        allowed = band_mask & (s * seq_rows + first + key_at >= WINDOW)
        scores = jnp.where(allowed, scores, -1e30)
        top = jnp.maximum(jnp.max(scores, axis=1, keepdims=True), sink)
        exps = jnp.exp(scores - top)
        total = jnp.sum(exps, axis=1, keepdims=True) + jnp.exp(sink - top)
        probs = (exps / total).astype(BF16)
        o = dot(probs, v_ext[pl.ds(first, rows + WINDOW), :])
        o0, o1 = o[0:rows], o[rows : 2 * rows]
        o0 = jnp.where(parity == 0, o0, pltpu.roll(o0, 64, 1))
        o1 = jnp.where(parity == 1, o1, pltpu.roll(o1, 64, 1))
        return jnp.where(lane_id < HD, o0, o1).astype(BF16)

    def head_rows(j):
        return remote(attended.at[j], heads.at[z], h_send.at[j], h_recv.at[j], z_peer(j))

    def attend_chip(i):
        j = (i + 1) % lanes
        other = (z + j) % lanes

        def half(n):
            value = attend(other * 2 + n)

            @pl.when(j > 0)
            def _():
                attended[j, pl.ds(pl.multiple_of(n * rows, rows), rows), :] = value

            @pl.when(j == 0)
            def _():
                heads[z, pl.ds(pl.multiple_of(n * rows, rows), rows), :] = value

        loop(2, half)

        @pl.when(j > 0)
        def _():
            head_rows(j).start()

    loop(lanes, attend_chip)

    for g in range(groups):
        for j in range(1, lanes):
            out_shard(g, j).wait_recv()
            for i in range(1, n_sp):
                out_relay(g, j, i).start()

    lane_q = lax.broadcasted_iota(jnp.int32, (1, seq_rows), 1)
    named_rows, weight_rows = [], []
    for j in range(n_sp):
        target = ((s + j) % n_sp * lanes + z).astype(F32)
        hit = info[0:TOPK] == target
        named_rows.append(jnp.max(jnp.where(hit, 1.0, 0.0), axis=0, keepdims=True))
        weight_rows.append(jnp.sum(jnp.where(hit, info[TOPK : 2 * TOPK], 0.0), axis=0, keepdims=True))
    fill = [jnp.zeros((1, seq_rows), F32)] * (-n_sp % 8)
    named = jnp.concatenate(named_rows + fill, axis=0)
    scan = named
    apart = 1
    while apart < seq_rows:
        scan = scan + jnp.where(lane_q >= apart, pltpu.roll(scan, apart, 1), 0.0)
        apart *= 2
    half_at = (core * half_cap).astype(F32)
    places = jnp.where(named > 0, scan - named - half_at, -1.0)
    for j in range(n_sp):
        place_t[j] = places[j : j + 1]
    place[...] = places.T.reshape(place.shape)
    weight[...] = jnp.concatenate(weight_rows + fill, axis=0).T.reshape(weight.shape)

    slot_down = lax.broadcasted_iota(jnp.int32, (half_cap, 1), 0).astype(F32)
    slot_along = lax.broadcasted_iota(jnp.int32, (1, half_cap), 1).astype(F32)

    def build_pick(j):
        hit = place_t[j] == slot_down
        onehot[j] = jnp.where(hit, 1.0, 0.0).astype(BF16)

    loop(n_sp, build_pick)

    def build_mix(i):
        for j in range(n_sp):
            hit = place[i, :, j : j + 1] == slot_along
            part = jnp.where(hit, weight[i, :, j : j + 1], 0.0).astype(BF16)
            mix[i, :, j * half_cap : (j + 1) * half_cap] = part

    loop(n_tp, build_mix)

    for j in range(1, lanes):
        head_rows(j).wait_recv()
    for g in range(groups):
        for j in range(1, lanes):
            for i in range(1, n_sp):
                out_relay(g, j, i).wait_recv()
    for c in range(chunks):
        out_own(c).wait()
    own_residual.wait()

    def stripe(c):
        return pl.ds(pl.multiple_of(c * per * rows, per * rows), per * rows)

    def exchange(c):
        return remote(
            acc_g.at[1 - core, stripe(c)], acc_g.at[2, stripe(c)], p_send.at[c], p_recv.at[c], partner
        )

    def project(c):
        parts = [
            dot(heads[i][:, 0:head_cols], wd[c, i * head_cols : (i + 1) * head_cols, :]) for i in range(lanes)
        ]
        value = sum(parts[1:], parts[0])
        for n in range(2):
            for p in range(per):
                at = pl.ds(pl.multiple_of((c * per + p) * rows, rows), rows)
                acc_g[n, at, :] = value[n * rows : (n + 1) * rows, p * TILE : (p + 1) * TILE]
        exchange(c).start()

    loop(chunks, project)
    for g in range(groups):
        for j in range(1, lanes):
            for i in range(1, n_sp):
                out_relay(g, j, i).wait_send()
    for c in range(chunks):
        own_weight(2, c).start()
    squares = jnp.zeros((rows, 1), F32)
    for c in range(chunks):
        exchange(c).wait_recv()
        for p in range(per):
            k = c * per + p
            at = pl.ds(k * rows, rows)
            band = slice(k * TILE, (k + 1) * TILE)
            value = after_mix[:, band].astype(F32) + (acc_g[core, at, :] + acc_g[2, at, :])
            value = value.astype(BF16)
            after_mix[:, band] = value
            squares += jnp.sum(value.astype(F32) * value.astype(F32), axis=1, keepdims=True)
    scale = lax.rsqrt(squares / width + 1e-06)
    for c in range(chunks):
        band = slice(c * step, (c + 1) * step)
        gathered[c, t] = (after_mix[:, band].astype(F32) * scale * gain[:, band]).astype(BF16)
        for j in range(1, lanes):
            own_piece(c, j).start()
        own_to_partner(c).start()
    for c in range(chunks):
        exchange(c).wait_send()

    def gather_chunk(c):
        for j in range(1, lanes):
            own_piece(c, j).wait_recv()
            forward(c, j).start()
        own_to_partner(c).wait_recv()
        for j in range(1, lanes):
            forward(c, j).wait_recv()

    def pick_chunk(c):
        block = gathered[c].reshape(n_tp * rows, step)

        def one(i):
            j = (i + 1) % n_sp
            value = dot(onehot[j], block).astype(BF16)

            @pl.when(j > 0)
            def _():
                sent[c, j] = value
                dispatch(c, j).start()

            @pl.when(j == 0)
            def _():
                arrived[c, j] = value

        loop(n_sp, one)

    def shared_chunk(c):
        for n in range(2):
            shared_weight(n, c).wait()
        block = gathered[c].reshape(n_tp * rows, step)
        value = dot_t(block, sgu[c])

        @pl.when(c == 0)
        def _():
            sh_acc[...] = value

        @pl.when(c > 0)
        def _():
            sh_acc[...] += value

    def expert_chunk(c):
        for n in range(2):
            own_weight(n, c).wait()
            other_weight(n, c).wait_recv()

        for j in range(1, n_sp):
            dispatch(c, j).wait_recv()
        lhs = arrived[c].reshape(slots, step)

        def one(i):
            band = pl.ds(pl.multiple_of(i * TILE, TILE), TILE)
            for w, acc in ((wg, acc_g), (wu, acc_u)):
                value = dot_t(lhs, w[c, band, :])

                @pl.when(c == 0)
                def _():
                    acc[i] = value

                @pl.when(c > 0)
                def _():
                    acc[i] += value

        loop(bands, one)

    def dispatch_step(c):
        gather_chunk(c)
        pick_chunk(c)
        shared_chunk(c)

        @pl.when(c > 0)
        def _():
            expert_chunk(c - 1)

    loop(chunks, dispatch_step)
    expert_chunk(chunks - 1)

    def activate(i):
        value = (silu(acc_g[i]) * acc_u[i]).astype(BF16).reshape(n_sp, half_cap, TILE)
        band = pl.ds(pl.multiple_of(i % per * TILE, TILE), TILE)
        arrived[i // per, :, :, band] = value

    loop(bands, activate)
    shared_value = silu(sh_acc[:, 0:sff]) * sh_acc[:, sff : 2 * sff]
    sh[...] = shared_value.astype(BF16).reshape(sh.shape)

    def settle_dispatch(c):
        for j in range(1, n_sp):
            dispatch(c, j).wait_send()
        for j in range(1, lanes):
            own_piece(c, j).wait_send()
            forward(c, j).wait_send()
        own_to_partner(c).wait_send()

    loop(chunks, settle_dispatch)

    def down_chunk(c):
        own_weight(2, c).wait()
        other_weight(2, c).wait_recv()

        def one(i):
            j = (i + 1) % n_sp
            parts = [
                dot(arrived[n, j], wd[c, n * step : (n + 1) * step, :]) for n in range(2 * ff // step)
            ]
            value = sum(parts[1:], parts[0]).astype(BF16)

            @pl.when(j > 0)
            def _():
                sent[c, j] = value
                give_back(c, j).start()

            @pl.when(j == 0)
            def _():
                returned[c, j] = value

        loop(n_sp, one)

    loop(chunks, down_chunk)

    def combine_chunk(c):
        shared_weight(2, c).wait()
        for j in range(1, n_sp):
            give_back(c, j).wait_recv()
        held = returned[c].reshape(slots, step)

        def part(i):
            return dot(mix[i], held) + dot(sh[i], sd[c])

        def away(i):
            gathered[c, i] = part(i * 2 + 1 - core).astype(BF16)

        loop(lanes, away)
        cross(c).start()
        cross(c).wait_recv()

        def home(i):
            j = (i + 1) % lanes
            other = (z + j) % lanes
            value = part(other * 2 + core) + x_recv[c, other].astype(F32)
            gathered[c, lanes + j] = value.astype(BF16)

            @pl.when(j > 0)
            def _():
                spread(c, j).start()

        loop(lanes, home)

    loop(chunks, combine_chunk)

    def finish_chunk(c):
        total = gathered[c, lanes].astype(F32)
        for j in range(1, lanes):
            spread(c, j).wait_recv()
        for j in range(1, lanes):
            total += z_recv[c, j].astype(F32)
        out[:, cols(c)] = (after_mix[:, cols(c)].astype(F32) + total).astype(BF16)

    loop(chunks, finish_chunk)

    def settle(c):
        for j in range(1, lanes):
            spread(c, j).wait_send()
        for j in range(1, n_sp):
            give_back(c, j).wait_send()
        for n in range(3):
            other_weight(n, c).wait_send()
        cross(c).wait_send()

    loop(chunks, settle)
    rim(keys, k_ext, 0).wait_send()
    rim(values, v_ext, 1).wait_send()
    for j in range(1, lanes):
        head_rows(j).wait_send()
        for g in range(groups):
            out_shard(g, j).wait_send()


def layer(
    queries, sinks, info, gain, keys, values, w_out, residual, w_gate, w_up, w_down, s_gate, s_up, s_down
):
    n_sp = lax.axis_size("sp")
    n_tp = lax.axis_size("tp")
    lanes = n_tp // 2
    rows, width = residual.shape
    step = width // CHUNKS
    ff = w_gate.shape[1]
    sff = s_gate.shape[0]
    q = rows * n_tp
    half_cap = max(2, 2 * q * TOPK // (n_sp * lanes)) // 2
    slots = n_sp * half_cap
    groups = width // min(width // n_sp, step) // n_sp
    padded = -(-n_sp // 8) * 8
    dma = pltpu.SemaphoreType.DMA
    vm = pltpu.VMEM
    in_vmem = pl.BlockSpec(memory_space=pltpu.VMEM)
    in_smem = pl.BlockSpec(memory_space=pltpu.SMEM)
    in_hbm = pl.BlockSpec(memory_space=pl.ANY)
    scratch = [
        vm((CHUNKS, 2 * ff, step), BF16),
        vm((CHUNKS, 2 * ff, step), BF16),
        vm((CHUNKS, 2 * ff, step), BF16),
        vm((CHUNKS, 2 * sff, step), BF16),
        vm((CHUNKS, sff, step), BF16),
        vm((CHUNKS, n_tp, rows, step), BF16),
        vm((n_sp, half_cap, q), BF16),
        vm((n_tp, rows, slots), BF16),
        vm((CHUNKS, n_sp, half_cap, step), BF16),
        vm((CHUNKS, n_sp, half_cap, step), BF16),
        vm((2 * ff // TILE, slots, TILE), F32),
        vm((2 * ff // TILE, slots, TILE), F32),
        vm((q, 2 * sff), F32),
        vm((n_tp, rows, sff), BF16),
        vm((CHUNKS, n_sp, half_cap, step), BF16),
        vm((CHUNKS, lanes, rows, step), BF16),
        vm((CHUNKS, lanes, rows, step), BF16),
        dma((3, CHUNKS)),
        dma((3, CHUNKS)),
        dma((3, CHUNKS)),
        dma((3, CHUNKS)),
        dma((CHUNKS, lanes)),
        dma((CHUNKS, lanes)),
        dma((CHUNKS, lanes)),
        dma((CHUNKS, lanes)),
        dma((CHUNKS, n_sp)),
        dma((CHUNKS, n_sp)),
        dma((CHUNKS, n_sp)),
        dma((CHUNKS, n_sp)),
        dma((CHUNKS,)),
        dma((CHUNKS,)),
        dma((CHUNKS, lanes)),
        dma((CHUNKS, lanes)),
        vm((q + WINDOW, 128), BF16),
        vm((q + WINDOW, 128), BF16),
        vm((lanes, 2 * rows, 128), BF16),
        vm((lanes, 2 * rows, 128), BF16),
        vm((rows, width), BF16),
        vm((n_sp, 1, q), F32),
        vm((n_tp, rows, padded), F32),
        vm((n_tp, rows, padded), F32),
        dma((4, CHUNKS)),
        dma((2,)),
        dma((2,)),
        dma((groups, lanes)),
        dma((groups, lanes)),
        dma((groups, lanes, n_sp)),
        dma((groups, lanes, n_sp)),
        dma((lanes,)),
        dma((lanes,)),
        dma((CHUNKS,)),
        dma((CHUNKS,)),
    ]
    return pl.pallas_call(
        layer_kernel,
        name="layer",
        out_shape=jax.ShapeDtypeStruct((rows, width), BF16),
        in_specs=[in_vmem, in_smem, in_vmem, in_vmem] + [in_hbm] * 10,
        out_specs=in_vmem,
        scratch_shapes=scratch,
        compiler_params=pltpu.CompilerParams(
            collective_id=0, has_side_effects=True, vmem_limit_bytes=67043328
        ),
        cost_estimate=pl.CostEstimate(
            flops=12 * slots * ff * width, bytes_accessed=6 * ff * width, transcendentals=0
        ),
    )(queries, sinks, info, gain, keys, values, w_out, residual, w_gate, w_up, w_down, s_gate, s_up, s_down)


def body(
    queries,
    keys,
    values,
    sink_logits,
    w_out,
    residual,
    norm_gain,
    expert_ids,
    expert_weights,
    w_gate,
    w_up,
    w_down,
    shared_gate,
    shared_up,
    shared_down,
):
    spare = 128 - queries.shape[1]
    if spare > 0:
        queries = jnp.pad(queries, ((0, 0), (0, spare)))
        sink_logits = jnp.pad(sink_logits, (0, spare // HD))
    info = jnp.concatenate([expert_ids.T.astype(F32), expert_weights.T], axis=0)
    return layer(
        queries,
        sink_logits,
        info,
        norm_gain[None],
        keys,
        values,
        w_out,
        residual,
        w_gate,
        w_up,
        w_down,
        shared_gate,
        shared_up,
        shared_down,
    )


def solution(mesh):
    return jax.shard_map(
        body,
        mesh=mesh,
        in_specs=(
            P("sp", "tp"),
            P("sp", None),
            P("sp", None),
            P("tp"),
            P("tp", None),
            P(("sp", "tp"), None),
            P(),
            P("sp", None),
            P("sp", None),
            P(("sp", "tp"), None, None),
            P(("sp", "tp"), None, None),
            P(("sp", "tp"), None, None),
            P("tp", None),
            P("tp", None),
            P("tp", None),
        ),
        out_specs=P(("sp", "tp"), None),
        check_vma=False,
    )
```

```python
import functools

import jax
import jax.numpy as jnp
from jax import lax
from jax.experimental import pallas as pl
from jax.experimental.pallas import tpu as pltpu
from jax.sharding import PartitionSpec as P

HD = 64
GROUP = 4
WINDOW = 128
TOPK = 4
CHUNKS = 8
TILE = 256
MESH = pl.DeviceIdType.MESH
F32 = jnp.float32
BF16 = jnp.bfloat16
NT = (((1,), (1,)), ((), ()))


def dot(a, b):
    return jnp.dot(a, b, preferred_element_type=F32)


def dot_t(a, b):
    return lax.dot_general(a, b, NT, preferred_element_type=F32)


def silu(v):
    return v / (1.0 + jnp.exp(jnp.minimum(-v, 87.0)))


def loop(n, body):
    lax.fori_loop(0, n, lambda i, carry: (body(i), carry)[1], 0)


def layer_kernel(
    queries,
    sinks,
    ids,
    route_weights,
    gain,
    keys,
    values,
    w_out,
    residual,
    w_gate,
    w_up,
    w_down,
    s_gate,
    s_up,
    s_down,
    out,
    wg,
    wu,
    wd,
    sgu,
    sd,
    gathered,
    onehot,
    mix,
    sent,
    arrived,
    hidden,
    acc_g,
    acc_u,
    sh_acc,
    sh,
    returned,
    x_recv,
    z_recv,
    sends,
    locals_,
    w_recv,
    ag_recv,
    fw_recv,
    d_recv,
    r_recv,
    x_recv_sem,
    z_recv_sem,
    rim_send,
    rim_recv,
    wz_recv,
    wx_send,
    wx_recv,
    p_recv,
    k_ext,
    v_ext,
    attended,
    heads,
    after_mix,
    place_t,
    place,
):
    n_sp = lax.axis_size("sp")
    n_tp = lax.axis_size("tp")
    lanes = n_tp // 2
    s = lax.axis_index("sp")
    t = lax.axis_index("tp")
    z = t // 2
    core = t % 2
    rows = after_mix.shape[0]
    width = after_mix.shape[1]
    head_cols = w_out.shape[0]
    seq_rows = n_tp * rows
    chunks, _, _, step = gathered.shape
    half_cap = sent.shape[2]
    slots = n_sp * half_cap
    ff = wg.shape[1] // 2
    sff = sd.shape[1]
    bands = 2 * ff // TILE
    per = step // TILE

    def sp_index(j):
        other, bit = s, 1
        while bit < n_sp:
            if j // bit % 2:
                other = other + bit - 2 * bit * (s // bit % 2)
            bit *= 2
        return other

    def sp_peer(j):
        return {"sp": sp_index(j)}

    def z_peer(j):
        return {"tp": ((z + j) % lanes) * 2 + core}

    partner = {"tp": z * 2 + 1 - core}

    barrier = pltpu.get_barrier_semaphore()
    for j in range(1, n_sp):
        pl.semaphore_signal(barrier, inc=1, device_id=sp_peer(j), device_id_type=MESH)
    for j in range(1, lanes):
        pl.semaphore_signal(barrier, inc=1, device_id=z_peer(j), device_id_type=MESH)
    pl.semaphore_signal(barrier, inc=1, device_id=partner, device_id_type=MESH)

    def cols(c):
        return pl.ds(pl.multiple_of(c * step, step), step)

    def remote(src, dst, send, recv, peer):
        return pltpu.make_async_remote_copy(
            src_ref=src, dst_ref=dst, send_sem=send, recv_sem=recv, device_id=peer, device_id_type=MESH
        )

    def wait_bytes(ref, sem):
        remote(ref, ref, sem, sem, partner).wait_recv()

    def is_far(j):
        gap = (z + j) % lanes - z
        return (gap * gap == (lanes - 1) ** 2) & (lanes > 2)

    def from_nearest(k):
        low = jnp.where(k >= z, k + 1, k)
        high = lanes - 1 - jnp.where(k >= lanes - 1 - z, k + 1, k)
        return jnp.where(2 * z < lanes, low, high)

    edge = (z % (lanes - 1) == 0) & (lanes > 2)
    relay_up = (z == lanes - 2) & (lanes > 2)
    relay_down = (z == 1) & (lanes > 2)

    def own_piece(c, j):
        return remote(gathered.at[c, t], gathered.at[c, t], sends.at[0], ag_recv.at[c, z], z_peer(j))

    def first_far(j):
        block = gathered.at[0, t]
        return remote(block, block, sends.at[13], ag_recv.at[0, z], z_peer(j))

    def own_to_partner(c):
        return remote(gathered.at[c, t], gathered.at[c, t], sends.at[1], fw_recv.at[c], partner)

    def forward(c, source):
        block = gathered.at[c, source * 2 + core]
        return remote(block, block, sends.at[1], fw_recv.at[c], partner)

    def relay_piece(c, source, to, n):
        block = gathered.at[c, source * 2 + core]
        return remote(block, block, sends.at[n], ag_recv.at[c, source], {"tp": to * 2 + core})

    def dispatch(c, j):
        sem = d_recv.at[c + c // (chunks - 1) * j]
        return remote(sent.at[c, j], arrived.at[c, j], sends.at[2], sem, sp_peer(j))

    def give_back(c, j):
        return remote(sent.at[c, j], returned.at[c, j], sends.at[3], r_recv.at[c], sp_peer(j))

    def cross(c):
        return remote(gathered.at[c, 0:lanes], x_recv.at[c], sends.at[4], x_recv_sem.at[c], partner)

    def spread(c, j):
        block = gathered.at[c, lanes + (z + j) % lanes]
        return remote(block, z_recv.at[c, j], sends.at[5], z_recv_sem.at[c], z_peer(j))

    weights = ((w_gate, wg), (w_up, wu), (w_down, wd))
    shared = (
        (s_gate, lambda c: sgu.at[c, 0:sff]),
        (s_up, lambda c: sgu.at[c, sff : 2 * sff]),
        (s_down, lambda c: sd.at[c]),
    )

    def own_weight(n, c):
        src, dst = weights[n]
        return pltpu.make_async_copy(src.at[0, :, cols(c)], dst.at[c, 0:ff], locals_.at[n // 2])

    def other_weight(n, c):
        src, dst = weights[n]
        block = dst.at[c, ff : 2 * ff]
        return remote(src.at[0, :, cols(c)], block, sends.at[6 + n // 2], w_recv.at[n // 2], partner)

    def shared_weight(n, c):
        src, dst = shared[n]
        return pltpu.make_async_copy(src.at[:, cols(c)], dst(c), locals_.at[2 + n // 2])

    group_width = min(width // n_sp, step)
    groups = width // group_width // n_sp

    def group_at(sp, g, lane):
        first = (sp * groups + g) * group_width
        band = pl.ds(pl.multiple_of(first % step, group_width), group_width)
        return wd.at[first // step, pl.ds(pl.multiple_of(lane * head_cols, head_cols), head_cols), band]

    def out_shard(g, j):
        block = group_at(s, g, z)
        return remote(block, block, sends.at[8], wz_recv.at[g, z], z_peer(j))

    def out_along(g, source, to, n):
        block = group_at(s, g, source)
        return remote(block, block, sends.at[n], wz_recv.at[g, source], {"tp": to * 2 + core})

    def out_relay(g, source, i):
        block = group_at(s, g, source)
        return remote(block, block, wx_send.at[i], wx_recv.at[i], sp_peer(i))

    some_pieces = wd.at[0:groups, 0 : (lanes - 1) * head_cols, 0:group_width]
    fewer_pieces = wd.at[0:groups, 0 : (lanes - 2) * head_cols, 0:group_width]
    relay_pieces = wd.at[0:groups, 0:head_cols, 0:group_width]

    def out_own(c):
        mine = wd.at[c, pl.ds(pl.multiple_of(z * head_cols, head_cols), head_cols)]
        return pltpu.make_async_copy(w_out.at[:, cols(c)], mine, locals_.at[4])

    kv_start = t * head_cols // HD // GROUP * HD
    kv_cols = pl.ds(pl.multiple_of(kv_start // 128 * 128, 128), 128)
    parity = kv_start // HD % 2

    def rim(src, dst, n):
        last = src.at[pl.ds(seq_rows - WINDOW, WINDOW), kv_cols]
        return remote(last, dst.at[0:WINDOW], rim_send.at[n], rim_recv.at[n], {"sp": (s + 1) % n_sp})

    def own_kv(src, dst, n):
        return pltpu.make_async_copy(src.at[:, kv_cols], dst.at[WINDOW : WINDOW + seq_rows], locals_.at[5 + n])

    own_residual = pltpu.make_async_copy(residual, after_mix, locals_.at[7])
    own_kv(keys, k_ext, 0).start()
    own_kv(values, v_ext, 1).start()
    own_residual.start()

    loop(chunks, lambda c: out_own(c).start())

    def start_local(c):
        for n in range(2):
            own_weight(n, c).start()
        for n in range(3):
            shared_weight(n, c).start()

    loop(chunks, start_local)

    pltpu.make_async_copy(wd.at[:, 0:head_cols], wd.at[:, 0:head_cols], locals_.at[4]).wait()
    pl.semaphore_wait(barrier, n_sp - 1 + lanes - 1 + 1)
    for g in range(groups):
        for j in range(1, lanes):

            @pl.when(jnp.logical_not(is_far(j)))
            def _():
                out_shard(g, j).start()

    rim(keys, k_ext, 0).start()
    rim(values, v_ext, 1).start()

    def start_other(c):
        for n in range(3):
            other_weight(n, c).start()

    loop(chunks, start_other)
    own_kv(keys, k_ext, 0).wait()
    own_kv(values, v_ext, 1).wait()

    lane_id = lax.broadcasted_iota(jnp.int32, (1, 128), 1)
    query_row = lax.broadcasted_iota(jnp.int32, (2 * rows, 1), 0)
    in_block = query_row % rows
    key_at = lax.broadcasted_iota(jnp.int32, (1, rows + WINDOW), 1)
    band_mask = (key_at <= in_block + WINDOW) & (key_at > in_block)
    sink = jnp.where(query_row < rows, sinks[0], sinks[1])

    def attend(block):
        first = pl.multiple_of(block * rows, rows)

        @pl.when(block == 0)
        def _():
            rim(keys, k_ext, 0).wait_recv()
            rim(values, v_ext, 1).wait_recv()

        q = queries[pl.ds(first, rows), :].astype(F32) * HD ** (-0.5)
        turned = pltpu.roll(q, 64, 1)
        mine = lane_id // HD == parity
        q0 = jnp.where(mine, jnp.where(parity == 0, q, turned), 0.0)
        q1 = jnp.where(mine, jnp.where(parity == 1, q, turned), 0.0)
        q2 = jnp.concatenate([q0, q1], axis=0).astype(BF16)
        scores = dot_t(q2, k_ext[pl.ds(first, rows + WINDOW), :])
        allowed = band_mask & (s * seq_rows + first + key_at >= WINDOW)
        scores = jnp.where(allowed, scores, -1e30)
        top = jnp.maximum(jnp.max(scores, axis=1, keepdims=True), sink)
        exps = jnp.exp(scores - top)
        total = jnp.sum(exps, axis=1, keepdims=True) + jnp.exp(sink - top)
        probs = (exps / total).astype(BF16)
        o = dot(probs, v_ext[pl.ds(first, rows + WINDOW), :])
        o0, o1 = o[0:rows], o[rows : 2 * rows]
        o0 = jnp.where(parity == 0, o0, pltpu.roll(o0, 64, 1))
        o1 = jnp.where(parity == 1, o1, pltpu.roll(o1, 64, 1))
        return jnp.where(lane_id < HD, o0, o1).astype(BF16)

    def head_rows(j):
        return remote(attended.at[j], heads.at[z], sends.at[9], rim_recv.at[2], z_peer(j))

    def attend_chip(i):
        j = (i + 1) % lanes
        other = (z + j) % lanes

        def half(n):
            value = attend(other * 2 + n)

            @pl.when(j > 0)
            def _():
                attended[j, pl.ds(pl.multiple_of(n * rows, rows), rows), :] = value

            @pl.when(j == 0)
            def _():
                heads[z, pl.ds(pl.multiple_of(n * rows, rows), rows), :] = value

        loop(2, half)

    loop(lanes, attend_chip)

    def relay_shards(k):
        source = from_nearest(k)
        for g in range(groups):
            wait_bytes(group_at(s, g, source), wz_recv.at[g, source])

            @pl.when(relay_up & (source == 0))
            def _():
                out_along(g, 0, lanes - 1, 10).start()

            @pl.when(relay_down & (source == lanes - 1))
            def _():
                out_along(g, lanes - 1, 0, 11).start()

            for i in range(n_sp - 1, 0, -1):
                out_relay(g, source, i).start()

    loop(lanes - 2, relay_shards)
    for j in range(1, lanes):
        head_rows(j).start()
    relay_shards(lanes - 2)

    lane_q = lax.broadcasted_iota(jnp.int32, (1, seq_rows), 1)
    named_rows, weight_rows = [], []
    for j in range(n_sp):
        hit = ids[...] == sp_index(j) * lanes + z
        named_rows.append(jnp.max(jnp.where(hit, 1.0, 0.0), axis=0, keepdims=True))
        weight_rows.append(jnp.sum(jnp.where(hit, route_weights[...], 0.0), axis=0, keepdims=True))
    fill = [jnp.zeros((1, seq_rows), F32)] * (-n_sp % 8)
    named = jnp.concatenate(named_rows + fill, axis=0)
    scan = named
    apart = 1
    while apart < seq_rows:
        scan = scan + jnp.where(lane_q >= apart, pltpu.roll(scan, apart, 1), 0.0)
        apart *= 2
    half_at = (core * half_cap).astype(F32)
    places = jnp.where(named > 0, scan - named - half_at, -1.0)
    for j in range(n_sp):
        place_t[j] = places[j : j + 1]
    place[...] = jnp.concatenate([places] + weight_rows + fill, axis=0).T.reshape(place.shape)

    slot_down = lax.broadcasted_iota(jnp.int32, (half_cap, 1), 0).astype(F32)
    slot_along = lax.broadcasted_iota(jnp.int32, (1, half_cap), 1).astype(F32)

    def build_pick(j):
        hit = place_t[j] == slot_down
        onehot[j] = jnp.where(hit, 1.0, 0.0).astype(BF16)

    loop(n_sp, build_pick)

    spot = places.shape[0]

    def build_mix(i):
        for j in range(n_sp):
            hit = place[i, :, j : j + 1] == slot_along
            part = jnp.where(hit, place[i, :, spot + j : spot + j + 1], 0.0).astype(BF16)
            at = pl.ds(pl.multiple_of(i // 2 * rows, rows), rows)
            mix[i % 2, at, j * half_cap : (j + 1) * half_cap] = part

    loop(n_tp, build_mix)


    wait_bytes(heads.at[1:lanes], rim_recv.at[2])
    own_residual.wait()

    def wait_relays(i):
        if i == 0:
            return
        wait_bytes(some_pieces, wx_recv.at[i])

    def stripe(c):
        return pl.ds(pl.multiple_of(c * per * rows, per * rows), per * rows)

    def exchange(c):
        return remote(
            acc_g.at[1 - core, stripe(c)], acc_g.at[2, stripe(c)], sends.at[12], p_recv.at[c], partner
        )

    def project(c):
        parts = [
            dot(heads[i][:, 0:head_cols], wd[c, i * head_cols : (i + 1) * head_cols, :]) for i in range(lanes)
        ]
        value = sum(parts[1:], parts[0])
        for n in range(2):
            for p in range(per):
                at = pl.ds(pl.multiple_of((c * per + p) * rows, rows), rows)
                acc_g[n, at, :] = value[n * rows : (n + 1) * rows, p * TILE : (p + 1) * TILE]
        exchange(c).start()

    if chunks % n_sp == 0:
        for i in range(n_sp):
            wait_relays(i)
            for n in range(chunks // n_sp):
                project(sp_index(i) * (chunks // n_sp) + n)
    else:
        for i in range(n_sp):
            wait_relays(i)
        loop(chunks, project)
    for i in range(1, n_sp):
        wait_bytes(some_pieces, wx_send.at[i])

    @pl.when(edge)
    def _():
        wait_bytes(fewer_pieces, sends.at[8])

    @pl.when(jnp.logical_not(edge))
    def _():
        wait_bytes(some_pieces, sends.at[8])

    @pl.when(relay_up)
    def _():
        wait_bytes(relay_pieces, sends.at[10])

    @pl.when(relay_down)
    def _():
        wait_bytes(relay_pieces, sends.at[11])

    for c in range(chunks):
        own_weight(2, c).start()
    def start_pieces(c):
        own_to_partner(c).start()
        for j in range(1, lanes):

            @pl.when(jnp.logical_not(is_far(j)))
            def _():
                own_piece(c, j).start()

            if isinstance(c, int) and c == 0:

                @pl.when(is_far(j))
                def _():
                    first_far(j).start()


    squares = jnp.zeros((rows, 1), F32)
    for c in range(chunks):
        exchange(c).wait_recv()
        for p in range(per):
            k = c * per + p
            at = pl.ds(k * rows, rows)
            band = slice(k * TILE, (k + 1) * TILE)
            value = after_mix[:, band].astype(F32) + (acc_g[core, at, :] + acc_g[2, at, :])
            value = value.astype(BF16)
            after_mix[:, band] = value
            squares += jnp.sum(value.astype(F32) * value.astype(F32), axis=1, keepdims=True)
    scale = lax.rsqrt(squares / width + 1e-06)
    for c in range(chunks):
        band = slice(c * step, (c + 1) * step)
        gathered[c, t] = (after_mix[:, band].astype(F32) * scale * gain[:, band]).astype(BF16)
        if c < 2:
            start_pieces(c)
    wait_bytes(acc_g.at[2, 0 : chunks * per * rows], sends.at[12])

    def gather_chunk(c):
        for k in range(lanes - 1):
            source = from_nearest(k)
            wait_bytes(gathered.at[c, source], ag_recv.at[c, source])

            @pl.when(relay_up & (source == 0) & (c > 0))
            def _():
                relay_piece(c, 0, lanes - 1, 10).start()

            @pl.when(relay_down & (source == lanes - 1) & (c > 0))
            def _():
                relay_piece(c, lanes - 1, 0, 11).start()

            forward(c, source).start()
        wait_bytes(gathered.at[c, 0:lanes], fw_recv.at[c])

    def pick_chunk(c):
        block = gathered[c].reshape(n_tp * rows, step)
        picked = dot(onehot[...].reshape(slots, seq_rows), block).astype(BF16)
        picked = picked.reshape(n_sp, half_cap, step)
        sent[c] = picked
        for j in range(n_sp - 1, 0, -1):
            dispatch(c, j).start()
        arrived[c, 0] = picked[0]

    def shared_chunk(c, first):
        block = gathered[c].reshape(n_tp * rows, step)
        value = dot_t(block, sgu[c])
        sh_acc[...] = value if first else sh_acc[...] + value

    def expert_chunk(c, first):
        wait_bytes(arrived.at[c, 1:n_sp], d_recv.at[c])
        lhs = arrived[c].reshape(slots, step)

        def one(i):
            band = pl.ds(pl.multiple_of(i * TILE, TILE), TILE)
            for w, acc in ((wg, acc_g), (wu, acc_u)):
                value = dot_t(lhs, w[c, band, :])
                acc[i] = value if first else acc[i] + value

        loop(bands, one)

    def last_rows(c, j):
        lhs = arrived[c, j]
        mine = slice(j * half_cap, (j + 1) * half_cap)
        for i in range(bands):
            band = slice(i * TILE, (i + 1) * TILE)
            g = acc_g[i, mine] + dot_t(lhs, wg[c, band, :])
            u = acc_u[i, mine] + dot_t(lhs, wu[c, band, :])
            hidden[j, :, band] = (silu(g) * u).astype(BF16)

    def dispatch_step(c, depth):
        gather_chunk(c)
        if isinstance(c, int):
            if c + 2 < chunks:
                start_pieces(c + 2)
        else:

            @pl.when(c + 2 < chunks)
            def _():
                start_pieces(c + 2)

        pick_chunk(c)
        shared_chunk(c, depth == 0)
        if depth > 1:
            expert_chunk(c - 2, depth == 2)

    def wait_local(ref, n):
        pltpu.make_async_copy(ref, ref, locals_.at[n]).wait()

    wait_local(sgu, 2)
    dispatch_step(0, 0)
    dispatch_step(1, 1)
    wait_local(wg, 0)
    wait_bytes(wg, w_recv.at[0])
    dispatch_step(2, 2)
    lax.fori_loop(3, chunks, lambda c, carry: (dispatch_step(c, 3), carry)[1], 0)
    expert_chunk(chunks - 2, False)
    shared_value = silu(sh_acc[:, 0:sff]) * sh_acc[:, sff : 2 * sff]
    shared_value = shared_value.astype(BF16)
    for i in range(n_tp):
        sh[i % 2, i // 2 * rows : (i // 2 + 1) * rows] = shared_value[i * rows : (i + 1) * rows]
    last_rows(chunks - 1, 0)

    wait_local(wd.at[:, 0:ff], 1)
    wait_bytes(wd.at[:, ff : 2 * ff], w_recv.at[1])
    for j in range(1, n_sp):
        dispatch(chunks - 1, j).wait_recv()
        last_rows(chunks - 1, j)
        if j == 1:
            wait_bytes(sent.at[:, 1:n_sp], sends.at[2])
        sent[0, j] = dot(hidden[j], wd[0]).astype(BF16)
        give_back(0, j).start()
    returned[0, 0] = dot(hidden[0], wd[0]).astype(BF16)

    def down_chunk(c):
        value = dot(hidden[...].reshape(slots, 2 * ff), wd[c]).astype(BF16)
        value = value.reshape(n_sp, half_cap, step)
        sent[c] = value
        for j in range(n_sp - 1, 0, -1):
            give_back(c, j).start()
        returned[c, 0] = value[0]

    down_chunk(1)
    wait_bytes(gathered.at[:, 0:lanes], sends.at[1])

    @pl.when(edge)
    def _():
        wait_bytes(gathered.at[:, 0 : lanes - 2], sends.at[0])
        wait_bytes(gathered.at[0, 0], sends.at[13])

    @pl.when(jnp.logical_not(edge))
    def _():
        wait_bytes(gathered.at[:, 0 : lanes - 1], sends.at[0])

    @pl.when(relay_up)
    def _():
        wait_bytes(gathered.at[1:chunks, 0], sends.at[10])

    @pl.when(relay_down)
    def _():
        wait_bytes(gathered.at[1:chunks, 0], sends.at[11])

    wait_local(sd, 3)

    def combine_chunk(c):
        wait_bytes(returned.at[c, 1:n_sp], r_recv.at[c])
        held = returned[c].reshape(slots, step)

        def part(p):
            return (dot(mix[p], held) + dot(sh[p], sd[c])).reshape(lanes, rows, step)

        gathered[c, 0:lanes] = part(1 - core).astype(BF16)
        cross(c).start()

        if c + 2 < chunks:
            down_chunk(c + 2)

        here = part(core)
        cross(c).wait_recv()
        gathered[c, lanes : 2 * lanes] = (here + x_recv[c].astype(F32)).astype(BF16)
        for j in range(1, lanes):
            spread(c, j).start()

    for c in range(chunks):
        combine_chunk(c)

    def finish_chunk(c):
        total = gathered[c, lanes + z].astype(F32)
        wait_bytes(z_recv.at[c, 1:lanes], z_recv_sem.at[c])
        for j in range(1, lanes):
            total += z_recv[c, j].astype(F32)
        out[:, cols(c)] = (after_mix[:, cols(c)].astype(F32) + total).astype(BF16)

    loop(chunks, finish_chunk)

    wait_bytes(gathered.at[:, 0 : lanes - 1], sends.at[5])
    wait_bytes(sent.at[:, 1:n_sp], sends.at[3])
    wait_bytes(gathered.at[:, 0:lanes], sends.at[4])
    wait_bytes(wg, sends.at[6])
    wait_bytes(wd.at[:, ff : 2 * ff], sends.at[7])
    wait_bytes(attended.at[1:lanes], sends.at[9])
    rim(keys, k_ext, 0).wait_send()
    rim(values, v_ext, 1).wait_send()


def layer(
    queries, sinks, ids, route_weights, gain, keys, values, w_out, residual, w_gate, w_up, w_down, s_gate, s_up, s_down
):
    n_sp = lax.axis_size("sp")
    n_tp = lax.axis_size("tp")
    lanes = n_tp // 2
    rows, width = residual.shape
    step = width // CHUNKS
    ff = w_gate.shape[1]
    sff = s_gate.shape[0]
    q = rows * n_tp
    half_cap = max(2, 2 * q * TOPK // (n_sp * lanes)) // 2
    slots = n_sp * half_cap
    groups = width // min(width // n_sp, step) // n_sp
    padded = -(-n_sp // 8) * 8
    dma = pltpu.SemaphoreType.DMA
    vm = pltpu.VMEM
    in_vmem = pl.BlockSpec(memory_space=pltpu.VMEM)
    in_smem = pl.BlockSpec(memory_space=pltpu.SMEM)
    in_hbm = pl.BlockSpec(memory_space=pl.ANY)
    scratch = [
        vm((CHUNKS, 2 * ff, step), BF16),
        vm((CHUNKS, 2 * ff, step), BF16),
        vm((CHUNKS, 2 * ff, step), BF16),
        vm((CHUNKS, 2 * sff, step), BF16),
        vm((CHUNKS, sff, step), BF16),
        vm((CHUNKS, n_tp, rows, step), BF16),
        vm((n_sp, half_cap, q), BF16),
        vm((2, lanes * rows, slots), BF16),
        vm((CHUNKS, n_sp, half_cap, step), BF16),
        vm((CHUNKS, n_sp, half_cap, step), BF16),
        vm((n_sp, half_cap, 2 * ff), BF16),
        vm((2 * ff // TILE, slots, TILE), F32),
        vm((2 * ff // TILE, slots, TILE), F32),
        vm((q, 2 * sff), F32),
        vm((2, lanes * rows, sff), BF16),
        vm((CHUNKS, n_sp, half_cap, step), BF16),
        vm((CHUNKS, lanes, rows, step), BF16),
        vm((CHUNKS, lanes, rows, step), BF16),
        dma((14,)),
        dma((8,)),
        dma((2,)),
        dma((CHUNKS, lanes)),
        dma((CHUNKS,)),
        dma((CHUNKS + n_sp,)),
        dma((CHUNKS,)),
        dma((CHUNKS,)),
        dma((CHUNKS,)),
        dma((2,)),
        dma((3,)),
        dma((groups, lanes)),
        dma((n_sp,)),
        dma((n_sp,)),
        dma((CHUNKS,)),
        vm((q + WINDOW, 128), BF16),
        vm((q + WINDOW, 128), BF16),
        vm((lanes, 2 * rows, 128), BF16),
        vm((lanes, 2 * rows, 128), BF16),
        vm((rows, width), BF16),
        vm((n_sp, 1, q), F32),
        vm((n_tp, rows, 2 * padded), F32),
    ]
    return pl.pallas_call(
        layer_kernel,
        name="layer",
        out_shape=jax.ShapeDtypeStruct((rows, width), BF16),
        in_specs=[in_vmem, in_smem, in_vmem, in_vmem, in_vmem] + [in_hbm] * 10,
        out_specs=in_vmem,
        scratch_shapes=scratch,
        compiler_params=pltpu.CompilerParams(
            collective_id=0, has_side_effects=True, vmem_limit_bytes=67043328
        ),
        cost_estimate=pl.CostEstimate(
            flops=12 * slots * ff * width, bytes_accessed=6 * ff * width, transcendentals=0
        ),
    )(queries, sinks, ids, route_weights, gain, keys, values, w_out, residual, w_gate, w_up, w_down, s_gate, s_up, s_down)


def body(
    queries,
    keys,
    values,
    sink_logits,
    w_out,
    residual,
    norm_gain,
    expert_ids,
    expert_weights,
    w_gate,
    w_up,
    w_down,
    shared_gate,
    shared_up,
    shared_down,
):
    spare = 128 - queries.shape[1]
    if spare > 0:
        queries = jnp.pad(queries, ((0, 0), (0, spare)))
        sink_logits = jnp.pad(sink_logits, (0, spare // HD))
    return layer(
        queries,
        sink_logits,
        expert_ids.T,
        expert_weights.T,
        norm_gain[None],
        keys,
        values,
        w_out,
        residual,
        w_gate,
        w_up,
        w_down,
        shared_gate,
        shared_up,
        shared_down,
    )


def solution(mesh):
    return jax.shard_map(
        body,
        mesh=mesh,
        in_specs=(
            P("sp", "tp"),
            P("sp", None),
            P("sp", None),
            P("tp"),
            P("tp", None),
            P(("sp", "tp"), None),
            P(),
            P("sp", None),
            P("sp", None),
            P(("sp", "tp"), None, None),
            P(("sp", "tp"), None, None),
            P(("sp", "tp"), None, None),
            P("tp", None),
            P("tp", None),
            P("tp", None),
        ),
        out_specs=P(("sp", "tp"), None),
        check_vma=False,
    )
```

```python
import functools

import jax
import jax.numpy as jnp
from jax import lax
from jax.experimental import pallas as pl
from jax.experimental.pallas import tpu as pltpu
from jax.sharding import PartitionSpec as P

HD = 64
GROUP = 4
WINDOW = 128
TOPK = 4
CHUNKS = 8
TILE = 256
MESH = pl.DeviceIdType.MESH
F32 = jnp.float32
BF16 = jnp.bfloat16
NT = (((1,), (1,)), ((), ()))


def dot(a, b):
    return jnp.dot(a, b, preferred_element_type=F32)


def dot_t(a, b):
    return lax.dot_general(a, b, NT, preferred_element_type=F32)


def silu(v):
    return v / (1.0 + jnp.exp(jnp.minimum(-v, 87.0)))


def loop(n, body):
    lax.fori_loop(0, n, lambda i, carry: (body(i), carry)[1], 0)


def layer_kernel(
    queries_in,
    sinks_in,
    ids_in,
    route_in,
    gain_in,
    keys,
    values,
    w_out,
    residual,
    w_gate,
    w_up,
    w_down,
    s_gate,
    s_up,
    s_down,
    out,
    wg,
    wu,
    wd,
    sgu,
    sd,
    gathered,
    onehot,
    mix,
    sent,
    arrived,
    hidden,
    acc_g,
    acc_u,
    sh_acc,
    sh,
    returned,
    x_recv,
    z_recv,
    sends,
    locals_,
    w_recv,
    ag_recv,
    fw_recv,
    d_recv,
    r_recv,
    x_recv_sem,
    z_recv_sem,
    rim_send,
    rim_recv,
    wz_recv,
    wx_send,
    wx_recv,
    p_recv,
    queries,
    sinks,
    ids,
    route_weights,
    gain,
    k_ext,
    v_ext,
    attended,
    heads,
    after_mix,
    place_t,
    place,
):
    n_sp = lax.axis_size("sp")
    n_tp = lax.axis_size("tp")
    lanes = n_tp // 2
    s = lax.axis_index("sp")
    t = lax.axis_index("tp")
    z = t // 2
    core = t % 2
    rows = after_mix.shape[0]
    width = after_mix.shape[1]
    head_cols = w_out.shape[0]
    seq_rows = n_tp * rows
    chunks, _, _, step = gathered.shape
    half_cap = sent.shape[2]
    slots = n_sp * half_cap
    ff = wg.shape[1] // 2
    sff = sd.shape[1]
    bands = 2 * ff // TILE
    per = step // TILE

    def sp_index(j):
        other, bit = s, 1
        while bit < n_sp:
            if j // bit % 2:
                other = other + bit - 2 * bit * (s // bit % 2)
            bit *= 2
        return other

    def sp_peer(j):
        return {"sp": sp_index(j)}

    def z_peer(j):
        return {"tp": ((z + j) % lanes) * 2 + core}

    partner = {"tp": z * 2 + 1 - core}

    barrier = pltpu.get_barrier_semaphore()
    for j in range(1, n_sp):
        pl.semaphore_signal(barrier, inc=1, device_id=sp_peer(j), device_id_type=MESH)
    for j in range(1, lanes):
        pl.semaphore_signal(barrier, inc=1, device_id=z_peer(j), device_id_type=MESH)
    pl.semaphore_signal(barrier, inc=1, device_id=partner, device_id_type=MESH)

    def cols(c):
        return pl.ds(pl.multiple_of(c * step, step), step)

    def remote(src, dst, send, recv, peer):
        return pltpu.make_async_remote_copy(
            src_ref=src, dst_ref=dst, send_sem=send, recv_sem=recv, device_id=peer, device_id_type=MESH
        )

    def wait_bytes(ref, sem):
        remote(ref, ref, sem, sem, partner).wait_recv()

    def is_far(j):
        gap = (z + j) % lanes - z
        return (gap * gap == (lanes - 1) ** 2) & (lanes > 2)

    def from_nearest(k):
        low = jnp.where(k >= z, k + 1, k)
        high = lanes - 1 - jnp.where(k >= lanes - 1 - z, k + 1, k)
        return jnp.where(2 * z < lanes, low, high)

    edge = (z % (lanes - 1) == 0) & (lanes > 2)
    relay_up = (z == lanes - 2) & (lanes > 2)
    relay_down = (z == 1) & (lanes > 2)

    def own_piece(c, j):
        return remote(gathered.at[c, t], gathered.at[c, t], sends.at[0], ag_recv.at[c, z], z_peer(j))

    def first_far(j):
        block = gathered.at[0, t]
        return remote(block, block, sends.at[13], ag_recv.at[0, z], z_peer(j))

    def own_to_partner(c):
        return remote(gathered.at[c, t], gathered.at[c, t], sends.at[1], fw_recv.at[c], partner)

    def forward(c, source):
        block = gathered.at[c, source * 2 + core]
        return remote(block, block, sends.at[1], fw_recv.at[c], partner)

    def relay_piece(c, source, to, n):
        block = gathered.at[c, source * 2 + core]
        return remote(block, block, sends.at[n], ag_recv.at[c, source], {"tp": to * 2 + core})

    def dispatch(c, j):
        sem = d_recv.at[c + c // (chunks - 1) * j]
        return remote(sent.at[c, j], arrived.at[c, j], sends.at[2], sem, sp_peer(j))

    def give_back(c, j):
        return remote(sent.at[c, j], returned.at[c, j], sends.at[3], r_recv.at[c], sp_peer(j))

    def cross(c):
        return remote(gathered.at[c, 0:lanes], x_recv.at[c], sends.at[4], x_recv_sem.at[c], partner)

    def spread(c, j):
        block = gathered.at[c, lanes + (z + j) % lanes]
        return remote(block, z_recv.at[c, j], sends.at[5], z_recv_sem.at[c], z_peer(j))

    weights = ((w_gate, wg), (w_up, wu), (w_down, wd))
    shared = (
        (s_gate, lambda c: sgu.at[c, 0:sff]),
        (s_up, lambda c: sgu.at[c, sff : 2 * sff]),
        (s_down, lambda c: sd.at[c]),
    )

    def own_weight(n, c):
        src, dst = weights[n]
        return pltpu.make_async_copy(src.at[0, :, cols(c)], dst.at[c, 0:ff], locals_.at[n // 2])

    def other_weight(n, c):
        src, dst = weights[n]
        block = dst.at[c, ff : 2 * ff]
        return remote(src.at[0, :, cols(c)], block, sends.at[6 + n // 2], w_recv.at[n // 2], partner)

    def shared_weight(n, c):
        src, dst = shared[n]
        return pltpu.make_async_copy(src.at[:, cols(c)], dst(c), locals_.at[2 + n // 2])

    group_width = min(width // n_sp, step)
    groups = width // group_width // n_sp

    def group_at(sp, g, lane):
        first = (sp * groups + g) * group_width
        band = pl.ds(pl.multiple_of(first % step, group_width), group_width)
        return wd.at[first // step, pl.ds(pl.multiple_of(lane * head_cols, head_cols), head_cols), band]

    def out_shard(g, j):
        block = group_at(s, g, z)
        return remote(block, block, sends.at[8], wz_recv.at[g, z], z_peer(j))

    def out_along(g, source, to, n):
        block = group_at(s, g, source)
        return remote(block, block, sends.at[n], wz_recv.at[g, source], {"tp": to * 2 + core})

    def out_relay(g, source, i):
        block = group_at(s, g, source)
        return remote(block, block, wx_send.at[i], wx_recv.at[i], sp_peer(i))

    some_pieces = wd.at[0:groups, 0 : (lanes - 1) * head_cols, 0:group_width]
    fewer_pieces = wd.at[0:groups, 0 : (lanes - 2) * head_cols, 0:group_width]
    relay_pieces = wd.at[0:groups, 0:head_cols, 0:group_width]

    def out_own(c):
        mine = wd.at[c, pl.ds(pl.multiple_of(z * head_cols, head_cols), head_cols)]
        return pltpu.make_async_copy(w_out.at[:, cols(c)], mine, locals_.at[4])

    kv_start = t * head_cols // HD // GROUP * HD
    kv_cols = pl.ds(pl.multiple_of(kv_start // 128 * 128, 128), 128)
    parity = kv_start // HD % 2

    def rim(src, dst, n):
        last = src.at[pl.ds(seq_rows - WINDOW, WINDOW), kv_cols]
        return remote(last, dst.at[0:WINDOW], rim_send.at[n], rim_recv.at[n], {"sp": (s + 1) % n_sp})

    def own_kv(src, dst, n):
        return pltpu.make_async_copy(src.at[:, kv_cols], dst.at[WINDOW : WINDOW + seq_rows], locals_.at[5 + n])

    own_residual = pltpu.make_async_copy(residual, after_mix, locals_.at[7])
    loop(chunks, lambda c: out_own(c).start())
    small = [
        pltpu.make_async_copy(src, dst, locals_.at[8 + n])
        for n, (src, dst) in enumerate(
            (
                (queries_in, queries),
                (sinks_in, sinks),
                (ids_in, ids),
                (route_in, route_weights),
                (gain_in, gain),
            )
        )
    ]
    for copy in small:
        copy.start()
    own_kv(keys, k_ext, 0).start()
    own_kv(values, v_ext, 1).start()
    own_residual.start()


    def start_local(c):
        for n in range(2):
            own_weight(n, c).start()
        for n in range(3):
            shared_weight(n, c).start()

    loop(chunks, start_local)

    pltpu.make_async_copy(wd.at[:, 0:head_cols], wd.at[:, 0:head_cols], locals_.at[4]).wait()
    pl.semaphore_wait(barrier, n_sp - 1 + lanes - 1 + 1)
    for g in range(groups):
        for j in range(1, lanes):

            @pl.when(jnp.logical_not(is_far(j)))
            def _():
                out_shard(g, j).start()

    rim(keys, k_ext, 0).start()
    rim(values, v_ext, 1).start()

    def start_other(c):
        for n in range(3):
            other_weight(n, c).start()

    loop(chunks, start_other)
    for copy in small:
        copy.wait()
    own_kv(keys, k_ext, 0).wait()
    own_kv(values, v_ext, 1).wait()

    lane_id = lax.broadcasted_iota(jnp.int32, (1, 128), 1)
    query_row = lax.broadcasted_iota(jnp.int32, (2 * rows, 1), 0)
    in_block = query_row % rows
    key_at = lax.broadcasted_iota(jnp.int32, (1, rows + WINDOW), 1)
    band_mask = (key_at <= in_block + WINDOW) & (key_at > in_block)
    sink = jnp.where(query_row < rows, sinks[:, 0:1], sinks[:, 1:2])

    def attend(block):
        first = pl.multiple_of(block * rows, rows)

        @pl.when(block == 0)
        def _():
            rim(keys, k_ext, 0).wait_recv()
            rim(values, v_ext, 1).wait_recv()

        q = queries[pl.ds(first, rows), :].astype(F32) * HD ** (-0.5)
        turned = pltpu.roll(q, 64, 1)
        mine = lane_id // HD == parity
        q0 = jnp.where(mine, jnp.where(parity == 0, q, turned), 0.0)
        q1 = jnp.where(mine, jnp.where(parity == 1, q, turned), 0.0)
        q2 = jnp.concatenate([q0, q1], axis=0).astype(BF16)
        scores = dot_t(q2, k_ext[pl.ds(first, rows + WINDOW), :])
        allowed = band_mask & (s * seq_rows + first + key_at >= WINDOW)
        scores = jnp.where(allowed, scores, -1e30)
        top = jnp.maximum(jnp.max(scores, axis=1, keepdims=True), sink)
        exps = jnp.exp(scores - top)
        total = jnp.sum(exps, axis=1, keepdims=True) + jnp.exp(sink - top)
        probs = (exps / total).astype(BF16)
        o = dot(probs, v_ext[pl.ds(first, rows + WINDOW), :])
        o0, o1 = o[0:rows], o[rows : 2 * rows]
        o0 = jnp.where(parity == 0, o0, pltpu.roll(o0, 64, 1))
        o1 = jnp.where(parity == 1, o1, pltpu.roll(o1, 64, 1))
        return jnp.where(lane_id < HD, o0, o1).astype(BF16)

    head_band = pl.ds(pl.multiple_of(z * 128, 128), 128)

    def head_rows(j):
        return remote(attended.at[j], heads.at[:, head_band], sends.at[9], rim_recv.at[2], z_peer(j))

    def attend_chip(i):
        j = (i + 1) % lanes
        other = (z + j) % lanes

        def half(n):
            value = attend(other * 2 + n)

            @pl.when(j > 0)
            def _():
                attended[j, pl.ds(pl.multiple_of(n * rows, rows), rows), :] = value

            @pl.when(j == 0)
            def _():
                heads[pl.ds(pl.multiple_of(n * rows, rows), rows), head_band] = value

        loop(2, half)

    loop(lanes - 1, attend_chip)

    def relay_shards(k):
        source = from_nearest(k)
        for g in range(groups):
            wait_bytes(group_at(s, g, source), wz_recv.at[g, source])

            @pl.when(relay_up & (source == 0))
            def _():
                out_along(g, 0, lanes - 1, 10).start()

            @pl.when(relay_down & (source == lanes - 1))
            def _():
                out_along(g, lanes - 1, 0, 11).start()

            for i in range(n_sp - 1, 0, -1):
                out_relay(g, source, i).start()

    relay_shards(0)
    loop(1, lambda i: attend_chip(i + lanes - 1))
    loop(lanes - 3, lambda k: relay_shards(k + 1))
    for j in range(1, lanes):
        head_rows(j).start()
    relay_shards(lanes - 2)

    lane_q = lax.broadcasted_iota(jnp.int32, (1, seq_rows), 1)
    named_rows, weight_rows = [], []
    for j in range(n_sp):
        hit = ids[...] == sp_index(j) * lanes + z
        named_rows.append(jnp.max(jnp.where(hit, 1.0, 0.0), axis=0, keepdims=True))
        weight_rows.append(jnp.sum(jnp.where(hit, route_weights[...], 0.0), axis=0, keepdims=True))
    fill = [jnp.zeros((1, seq_rows), F32)] * (-n_sp % 8)
    named = jnp.concatenate(named_rows + fill, axis=0)
    scan = named
    apart = 1
    while apart < seq_rows:
        scan = scan + jnp.where(lane_q >= apart, pltpu.roll(scan, apart, 1), 0.0)
        apart *= 2
    half_at = (core * half_cap).astype(F32)
    places = jnp.where(named > 0, scan - named - half_at, -1.0)
    for j in range(n_sp):
        place_t[j] = places[j : j + 1]
    place[...] = jnp.concatenate([places] + weight_rows + fill, axis=0).T.reshape(place.shape)

    slot_down = lax.broadcasted_iota(jnp.int32, (half_cap, 1), 0).astype(F32)
    slot_along = lax.broadcasted_iota(jnp.int32, (1, half_cap), 1).astype(F32)

    def build_pick(j):
        hit = place_t[j] == slot_down
        onehot[j] = jnp.where(hit, 1.0, 0.0).astype(BF16)

    loop(n_sp, build_pick)

    spot = places.shape[0]

    def build_mix(i):
        for j in range(n_sp):
            hit = place[i, :, j : j + 1] == slot_along
            part = jnp.where(hit, place[i, :, spot + j : spot + j + 1], 0.0).astype(BF16)
            at = pl.ds(pl.multiple_of(i // 2 * rows, rows), rows)
            mix[i % 2, at, j * half_cap : (j + 1) * half_cap] = part

    loop(n_tp, build_mix)


    wait_bytes(heads.at[:, 0 : (lanes - 1) * 128], rim_recv.at[2])
    own_residual.wait()

    def wait_relays(i):
        if i == 0:
            return
        wait_bytes(some_pieces, wx_recv.at[i])

    def stripe(c):
        return pl.ds(pl.multiple_of(c * per * rows, per * rows), per * rows)

    def exchange(c):
        return remote(
            acc_g.at[1 - core, stripe(c)], acc_g.at[2, stripe(c)], sends.at[12], p_recv.at[c], partner
        )

    def project(c):
        if head_cols == 128:
            value = dot(heads[...], wd[c, 0 : lanes * head_cols, :])
        else:
            parts = [
                dot(
                    heads[:, i * 128 : i * 128 + head_cols],
                    wd[c, i * head_cols : (i + 1) * head_cols, :],
                )
                for i in range(lanes)
            ]
            value = sum(parts[1:], parts[0])
        for n in range(2):
            for p in range(per):
                at = pl.ds(pl.multiple_of((c * per + p) * rows, rows), rows)
                acc_g[n, at, :] = value[n * rows : (n + 1) * rows, p * TILE : (p + 1) * TILE]
        exchange(c).start()

    if chunks % n_sp == 0:
        for i in range(n_sp):
            wait_relays(i)
            for n in range(chunks // n_sp):
                project(sp_index(i) * (chunks // n_sp) + n)
    else:
        for i in range(n_sp):
            wait_relays(i)
        loop(chunks, project)
    for i in range(1, n_sp):
        wait_bytes(some_pieces, wx_send.at[i])

    @pl.when(edge)
    def _():
        wait_bytes(fewer_pieces, sends.at[8])

    @pl.when(jnp.logical_not(edge))
    def _():
        wait_bytes(some_pieces, sends.at[8])

    @pl.when(relay_up)
    def _():
        wait_bytes(relay_pieces, sends.at[10])

    @pl.when(relay_down)
    def _():
        wait_bytes(relay_pieces, sends.at[11])

    for c in range(chunks):
        own_weight(2, c).start()
    def start_pieces(c):
        own_to_partner(c).start()
        for j in range(1, lanes):

            @pl.when(jnp.logical_not(is_far(j)))
            def _():
                own_piece(c, j).start()

            if isinstance(c, int) and c == 0:

                @pl.when(is_far(j))
                def _():
                    first_far(j).start()


    squares = jnp.zeros((rows, 1), F32)
    for c in range(chunks):
        exchange(c).wait_recv()
        for p in range(per):
            k = c * per + p
            at = pl.ds(k * rows, rows)
            band = slice(k * TILE, (k + 1) * TILE)
            value = after_mix[:, band].astype(F32) + (acc_g[core, at, :] + acc_g[2, at, :])
            value = value.astype(BF16)
            after_mix[:, band] = value
            squares += jnp.sum(value.astype(F32) * value.astype(F32), axis=1, keepdims=True)
    scale = lax.rsqrt(squares / width + 1e-06)
    for c in range(chunks):
        band = slice(c * step, (c + 1) * step)
        gathered[c, t] = (after_mix[:, band].astype(F32) * scale * gain[:, band]).astype(BF16)
        if c < 2:
            start_pieces(c)
    wait_bytes(acc_g.at[2, 0 : chunks * per * rows], sends.at[12])

    def gather_chunk(c):
        for k in range(lanes - 1):
            source = from_nearest(k)
            wait_bytes(gathered.at[c, source], ag_recv.at[c, source])

            @pl.when(relay_up & (source == 0) & (c > 0))
            def _():
                relay_piece(c, 0, lanes - 1, 10).start()

            @pl.when(relay_down & (source == lanes - 1) & (c > 0))
            def _():
                relay_piece(c, lanes - 1, 0, 11).start()

            forward(c, source).start()
        wait_bytes(gathered.at[c, 0:lanes], fw_recv.at[c])

    def pick_chunk(c):
        block = gathered[c].reshape(n_tp * rows, step)
        picked = dot(onehot[...].reshape(slots, seq_rows), block).astype(BF16)
        picked = picked.reshape(n_sp, half_cap, step)
        sent[c] = picked
        for j in range(n_sp - 1, 0, -1):
            dispatch(c, j).start()
        arrived[c, 0] = picked[0]

    def shared_chunk(c, first):
        block = gathered[c].reshape(n_tp * rows, step)
        value = dot_t(block, sgu[c])
        sh_acc[...] = value if first else sh_acc[...] + value

    def expert_chunk(c, first):
        wait_bytes(arrived.at[c, 1:n_sp], d_recv.at[c])
        lhs = arrived[c].reshape(slots, step)

        def one(i):
            band = pl.ds(pl.multiple_of(i * TILE, TILE), TILE)
            for w, acc in ((wg, acc_g), (wu, acc_u)):
                value = dot_t(lhs, w[c, band, :])
                acc[i] = value if first else acc[i] + value

        loop(bands, one)

    def last_rows(c, j):
        lhs = arrived[c, j]
        mine = slice(j * half_cap, (j + 1) * half_cap)
        for i in range(bands):
            band = slice(i * TILE, (i + 1) * TILE)
            g = acc_g[i, mine] + dot_t(lhs, wg[c, band, :])
            u = acc_u[i, mine] + dot_t(lhs, wu[c, band, :])
            hidden[j, :, band] = (silu(g) * u).astype(BF16)

    def dispatch_step(c, depth):
        gather_chunk(c)
        if isinstance(c, int):
            if c + 2 < chunks:
                start_pieces(c + 2)
        else:

            @pl.when(c + 2 < chunks)
            def _():
                start_pieces(c + 2)

        pick_chunk(c)
        shared_chunk(c, depth == 0)
        if depth > 1:
            expert_chunk(c - 2, depth == 2)

    def wait_local(ref, n):
        pltpu.make_async_copy(ref, ref, locals_.at[n]).wait()

    wait_local(sgu, 2)
    dispatch_step(0, 0)
    dispatch_step(1, 1)
    wait_local(wg, 0)
    wait_bytes(wg, w_recv.at[0])
    dispatch_step(2, 2)
    lax.fori_loop(3, chunks, lambda c, carry: (dispatch_step(c, 3), carry)[1], 0)
    expert_chunk(chunks - 2, False)
    shared_value = silu(sh_acc[:, 0:sff]) * sh_acc[:, sff : 2 * sff]
    shared_value = shared_value.astype(BF16)
    for i in range(n_tp):
        sh[i % 2, i // 2 * rows : (i // 2 + 1) * rows] = shared_value[i * rows : (i + 1) * rows]
    last_rows(chunks - 1, 0)

    wait_local(wd.at[:, 0:ff], 1)
    wait_bytes(wd.at[:, ff : 2 * ff], w_recv.at[1])
    for j in range(1, n_sp):
        dispatch(chunks - 1, j).wait_recv()
        last_rows(chunks - 1, j)
        if j == 1:
            wait_bytes(sent.at[:, 1:n_sp], sends.at[2])
        sent[0, j] = dot(hidden[j], wd[0]).astype(BF16)
        give_back(0, j).start()
    returned[0, 0] = dot(hidden[0], wd[0]).astype(BF16)

    def down_chunk(c):
        value = dot(hidden[...].reshape(slots, 2 * ff), wd[c]).astype(BF16)
        value = value.reshape(n_sp, half_cap, step)
        sent[c] = value
        for j in range(n_sp - 1, 0, -1):
            give_back(c, j).start()
        returned[c, 0] = value[0]

    down_chunk(1)
    wait_bytes(gathered.at[:, 0:lanes], sends.at[1])

    @pl.when(edge)
    def _():
        wait_bytes(gathered.at[:, 0 : lanes - 2], sends.at[0])
        wait_bytes(gathered.at[0, 0], sends.at[13])

    @pl.when(jnp.logical_not(edge))
    def _():
        wait_bytes(gathered.at[:, 0 : lanes - 1], sends.at[0])

    @pl.when(relay_up)
    def _():
        wait_bytes(gathered.at[1:chunks, 0], sends.at[10])

    @pl.when(relay_down)
    def _():
        wait_bytes(gathered.at[1:chunks, 0], sends.at[11])

    wait_local(sd, 3)

    def combine_chunk(c):
        wait_bytes(returned.at[c, 1:n_sp], r_recv.at[c])
        held = returned[c].reshape(slots, step)

        def part(p):
            return (dot(mix[p], held) + dot(sh[p], sd[c])).reshape(lanes, rows, step)

        gathered[c, 0:lanes] = part(1 - core).astype(BF16)
        cross(c).start()

        if c + 2 < chunks:
            down_chunk(c + 2)

        here = part(core)
        cross(c).wait_recv()
        gathered[c, lanes : 2 * lanes] = (here + x_recv[c].astype(F32)).astype(BF16)
        for j in range(1, lanes):
            spread(c, j).start()

    for c in range(chunks):
        combine_chunk(c)

    def finish_chunk(c):
        total = gathered[c, lanes + z].astype(F32)
        wait_bytes(z_recv.at[c, 1:lanes], z_recv_sem.at[c])
        for j in range(1, lanes):
            total += z_recv[c, j].astype(F32)
        out[:, cols(c)] = (after_mix[:, cols(c)].astype(F32) + total).astype(BF16)

    loop(chunks, finish_chunk)

    wait_bytes(gathered.at[:, 0 : lanes - 1], sends.at[5])
    wait_bytes(sent.at[:, 1:n_sp], sends.at[3])
    wait_bytes(gathered.at[:, 0:lanes], sends.at[4])
    wait_bytes(wg, sends.at[6])
    wait_bytes(wd.at[:, ff : 2 * ff], sends.at[7])
    wait_bytes(attended.at[1:lanes], sends.at[9])
    rim(keys, k_ext, 0).wait_send()
    rim(values, v_ext, 1).wait_send()


def layer(
    queries, sinks, ids, route_weights, gain, keys, values, w_out, residual, w_gate, w_up, w_down, s_gate, s_up, s_down
):
    n_sp = lax.axis_size("sp")
    n_tp = lax.axis_size("tp")
    lanes = n_tp // 2
    rows, width = residual.shape
    step = width // CHUNKS
    ff = w_gate.shape[1]
    sff = s_gate.shape[0]
    q = rows * n_tp
    half_cap = max(2, 2 * q * TOPK // (n_sp * lanes)) // 2
    slots = n_sp * half_cap
    groups = width // min(width // n_sp, step) // n_sp
    padded = -(-n_sp // 8) * 8
    dma = pltpu.SemaphoreType.DMA
    vm = pltpu.VMEM
    in_vmem = pl.BlockSpec(memory_space=pltpu.VMEM)
    in_hbm = pl.BlockSpec(memory_space=pl.ANY)
    scratch = [
        vm((CHUNKS, 2 * ff, step), BF16),
        vm((CHUNKS, 2 * ff, step), BF16),
        vm((CHUNKS, 2 * ff, step), BF16),
        vm((CHUNKS, 2 * sff, step), BF16),
        vm((CHUNKS, sff, step), BF16),
        vm((CHUNKS, n_tp, rows, step), BF16),
        vm((n_sp, half_cap, q), BF16),
        vm((2, lanes * rows, slots), BF16),
        vm((CHUNKS, n_sp, half_cap, step), BF16),
        vm((CHUNKS, n_sp, half_cap, step), BF16),
        vm((n_sp, half_cap, 2 * ff), BF16),
        vm((2 * ff // TILE, slots, TILE), F32),
        vm((2 * ff // TILE, slots, TILE), F32),
        vm((q, 2 * sff), F32),
        vm((2, lanes * rows, sff), BF16),
        vm((CHUNKS, n_sp, half_cap, step), BF16),
        vm((CHUNKS, lanes, rows, step), BF16),
        vm((CHUNKS, lanes, rows, step), BF16),
        dma((14,)),
        dma((13,)),
        dma((2,)),
        dma((CHUNKS, lanes)),
        dma((CHUNKS,)),
        dma((CHUNKS + n_sp,)),
        dma((CHUNKS,)),
        dma((CHUNKS,)),
        dma((CHUNKS,)),
        dma((2,)),
        dma((3,)),
        dma((groups, lanes)),
        dma((n_sp,)),
        dma((n_sp,)),
        dma((CHUNKS,)),
        vm((q, 128), BF16),
        vm((1, 2), F32),
        vm((TOPK, q), jnp.int32),
        vm((TOPK, q), F32),
        vm((1, width), F32),
        vm((q + WINDOW, 128), BF16),
        vm((q + WINDOW, 128), BF16),
        vm((lanes, 2 * rows, 128), BF16),
        vm((2 * rows, lanes * 128), BF16),
        vm((rows, width), BF16),
        vm((n_sp, 1, q), F32),
        vm((n_tp, rows, 2 * padded), F32),
    ]
    return pl.pallas_call(
        layer_kernel,
        name="layer",
        out_shape=jax.ShapeDtypeStruct((rows, width), BF16),
        in_specs=[in_hbm] * 15,
        out_specs=in_vmem,
        scratch_shapes=scratch,
        compiler_params=pltpu.CompilerParams(
            collective_id=0, has_side_effects=True, vmem_limit_bytes=67043328
        ),
        cost_estimate=pl.CostEstimate(
            flops=12 * slots * ff * width, bytes_accessed=6 * ff * width, transcendentals=0
        ),
    )(queries, sinks, ids, route_weights, gain, keys, values, w_out, residual, w_gate, w_up, w_down, s_gate, s_up, s_down)


def body(
    queries,
    keys,
    values,
    sink_logits,
    w_out,
    residual,
    norm_gain,
    expert_ids,
    expert_weights,
    w_gate,
    w_up,
    w_down,
    shared_gate,
    shared_up,
    shared_down,
):
    spare = 128 - queries.shape[1]
    if spare > 0:
        queries = jnp.pad(queries, ((0, 0), (0, spare)))
        sink_logits = jnp.pad(sink_logits, (0, spare // HD))
    return layer(
        queries,
        sink_logits[None],
        expert_ids.T,
        expert_weights.T,
        norm_gain[None],
        keys,
        values,
        w_out,
        residual,
        w_gate,
        w_up,
        w_down,
        shared_gate,
        shared_up,
        shared_down,
    )


def solution(mesh):
    return jax.shard_map(
        body,
        mesh=mesh,
        in_specs=(
            P("sp", "tp"),
            P("sp", None),
            P("sp", None),
            P("tp"),
            P("tp", None),
            P(("sp", "tp"), None),
            P(),
            P("sp", None),
            P("sp", None),
            P(("sp", "tp"), None, None),
            P(("sp", "tp"), None, None),
            P(("sp", "tp"), None, None),
            P("tp", None),
            P("tp", None),
            P("tp", None),
        ),
        out_specs=P(("sp", "tp"), None),
        check_vma=False,
    )
```
